256 devices in a mesh: ep: 16 (over y, x), tp: 16 (over z, core).
Axes of the slice: x: 4, y: 4, z: 8, core: 2. Of those that a mesh axis runs over, the one named last changes fastest.
Arguments:
- mixer_input_rows: bfloat16 [32768, 2048], P(('ep', 'tp')), may hold values from -6 to 6
- mixer_norm_gain: float32 [2048], replicated, may hold values from 0.1 to 1.9
- query_weight: bfloat16 [2048, 2048], P(None, 'tp'), may hold values from -0.125 to 0.125
- key_weight: bfloat16 [2048, 2048], P(None, 'tp'), may hold values from -0.125 to 0.125
- value_weight: bfloat16 [2048, 2048], P(None, 'tp'), may hold values from -0.125 to 0.125
- write_strength_projection: bfloat16 [2048, 16], replicated, may hold values from -0.125 to 0.125
- decay_projection: bfloat16 [2048, 16], replicated, may hold values from -0.125 to 0.125
- head_decay_speed: float32 [16], P('tp'), may hold values from 0 to 1
- largest_write_strength: float32 [16], P('tp'), may hold values from 0 to 1
- extra_log_decay: float32 [32768, 16], P('ep', 'tp'), may hold values from -1 to 0
- head_norm_gain: float32 [128], replicated, may hold values from 0.1 to 1.9
- mixer_output_weight: bfloat16 [2048, 2048], P('tp'), may hold values from -0.125 to 0.125
- expert_input_rows: bfloat16 [2048, 2048], P(('ep', 'tp')), may hold values from -6 to 6
- expert_norm_gain: float32 [2048], replicated, may hold values from 0.1 to 1.9
- routes: int32 [2048, 2], P(('ep', 'tp')), may hold values from 0 to 15, all different within a row; in each aligned block of 8 rows (0 to 7, 8 to 15, ...) at most 2 rows name the same one
- expert_route_weight: float32 [2048, 2], P(('ep', 'tp')), may hold values from 0.2 to 1
- gate_weight: bfloat16 [16, 2048, 7168], P('ep', None, 'tp'), may hold values from -0.125 to 0.125
- up_weight: bfloat16 [16, 2048, 7168], P('ep', None, 'tp'), may hold values from -0.125 to 0.125
- down_weight: bfloat16 [16, 7168, 2048], P('ep', 'tp'), may hold values from -0.0625 to 0.0625
Outputs:
- mix_out: bfloat16 [32768, 2048], P(('ep', 'tp'))
- exp_out: bfloat16 [2048, 2048], P(('ep', 'tp'))
The draws below stay inside these ranges and needn't reach their ends.
Inputs may be any that keep to these rules, and one draw needn't show every extreme that they name: `routes`: within the rows of one device (aligned blocks of 8 rows) no expert is named more than 2 times, some device names some expert exactly 2 times, and the 2 experts of a row differ.
All inputs are finite; a program needn't handle non-finite values.
Results may differ from the reference program's by a relative error of at most 0.019.
Values may be sent and summed in bfloat16 or wider, within the bound.
A program may use at most 128 MiB of HBM per device.

```python
import math
import jax
import jax.numpy as jnp
import numpy as np
from jax import lax

D = 2048
HEADS = 16
HEAD = 128
FF = 7168
BLOCK = 128
TOP = 2
EXP_TOK_DEV = 8
HEADS_DEV = 1
FF_DEV = 448
SPAN_EP = 2048
SEQ = 32768
EXP_TOKENS = 2048
EXPERTS = 16
CAP = 2
N_EP = 16
N_TP = 16


def head_split(key):
    ranks = jax.random.permutation(jax.random.fold_in(key, 101), HEADS)
    quick_count = HEADS // 2
    return ranks < quick_count


def draw_head_decay_speed(key, part):
    quick = head_split(key)
    fast_rate = jax.random.uniform(jax.random.fold_in(key, 102), (HEADS,), jnp.float32, 0.025, 0.05)
    slow_rate = jax.random.uniform(jax.random.fold_in(key, 103), (HEADS,), jnp.float32, 0.1, 0.3) / SEQ
    return jnp.where(quick, fast_rate, slow_rate)


def draw_largest_write_strength(key, part):
    quick = head_split(key)
    fast_rate = jax.random.uniform(jax.random.fold_in(key, 104), (HEADS,), jnp.float32, 0.6, 1.0)
    slow_rate = jax.random.uniform(jax.random.fold_in(key, 105), (HEADS,), jnp.float32, 0.5, 1.0) * HEAD / SEQ
    return jnp.where(quick, fast_rate, slow_rate)


def draw_extra_log_decay(key, part):
    span_count = SEQ // SPAN_EP
    position = jnp.arange(SEQ)
    steady = jax.random.uniform(jax.random.fold_in(key, 111), (span_count, HEADS), jnp.float32, 0.12, 0.5)
    level = -steady[position // SPAN_EP] / SEQ
    spots = jax.random.randint(jax.random.fold_in(key, 112), (3,), 0, SEQ)
    drops = jnp.log(jax.random.uniform(jax.random.fold_in(key, 113), (3, HEADS), jnp.float32, 0.6, 0.8))
    hits = (position[:, None] == spots[None, :]).astype(jnp.float32)
    return level + jnp.sum(hits[:, :, None] * drops[None, :, :], axis=1)


def shard_levels(own_key, extent, shards, smallest, top_value):
    factor_of, own = 1.0, jax.random.fold_in(own_key, 6)
    for dim, shards_of in shards:
        steps = jnp.exp(jax.random.uniform(jax.random.fold_in(own, dim), (shards_of,), jnp.float32, smallest / len(shards), top_value / len(shards)))
        factor_of = factor_of * jnp.repeat(steps, extent[dim] // shards_of).reshape([-1 if axis == dim else 1 for axis in range(len(extent))])
    return factor_of


def routed_block(stream_key, own, number, rows, count, top, limit, slope):
    order = jax.random.permutation(stream_key, count)
    packed, common = load_shares(count, rows * top, limit, slope, True), load_shares(count, rows * top, limit, slope, False)
    places = jnp.arange(count)

    def named(tallies, offset_by):
        used = int((tallies > 0).sum())
        fixed = max(1, used // 4)
        passed = fixed + (places - fixed + offset_by * (used - fixed)) % max(1, count - fixed)
        return jnp.zeros((count,), jnp.int32).at[order[jnp.where(places < fixed, places, passed)]].set(jnp.asarray(tallies, jnp.int32))

    tallies = jnp.where(number % 4 == 0, named(packed, number // 4), named(common, number - number // 4 - 1))
    mixed = jax.random.permutation(jax.random.fold_in(own, 3), count)
    source_of, taker = mixed[0:count // 2 * 2:2], mixed[1:count // 2 * 2:2]
    margin = jnp.minimum(tallies[source_of] - 1, limit - tallies[taker]) // 2
    margin = jnp.where((source_of == order[0]) | (taker == order[0]) | (tallies[taker] == 0), 0, jnp.maximum(margin, 0))
    passed = jax.random.randint(jax.random.fold_in(own, 4), (count // 2,), 0, 1 << 20) % (margin + 1)
    tallies = tallies.at[source_of].add(-passed).at[taker].add(passed)
    members = jnp.searchsorted(jnp.cumsum(tallies), jnp.arange(rows * top), side="right").astype(jnp.int32)
    listing = members.reshape(top, rows).T
    listing = listing[jax.random.permutation(jax.random.fold_in(own, 1), rows)]
    offset_by = jax.random.randint(jax.random.fold_in(own, 2), (rows, 1), 0, top)
    return jnp.take_along_axis(listing, (jnp.arange(top)[None, :] + offset_by) % top, axis=1)


def load_shares(number_of, total, reach, lean, full):
    portions = [(1 << 20) // math.isqrt(rank ** lean) + 1 for rank in range(1, number_of + 1)]
    largest = reach if full else min(reach, max(-(-total // number_of), total * portions[0] // sum(portions)))
    least = 1 if total - largest >= number_of - 1 else 0
    counts, spare = [largest] + [least] * (number_of - 1), total - largest - least * (number_of - 1)
    while spare > 0:
        free = [i for i in range(1, number_of) if counts[i] < largest] or [i for i in range(1, number_of) if counts[i] < reach]
        pool, remaining = sum([portions[i] for i in free]), spare
        for i in free:
            more = min(reach - counts[i], max(1, remaining * portions[i] // pool), spare)
            counts[i] = counts[i] + more
            spare = spare - more
    return np.array(counts)


def scatter_about(own_key, extent, scale, bound, cuts=(), kind=jnp.bfloat16):
    level = shard_levels(own_key, extent, cuts, -0.22, 0.18) if cuts else 1.0
    array = jax.random.normal(own_key, extent, jnp.float32) * scale * level
    return jnp.minimum(jnp.maximum(array, -bound), bound).astype(kind)


def setup_inputs(seed: int = 0) -> dict:
    streams_of = jax.random.split(jax.random.key(seed), 20)
    mixer_input_rows = scatter_about(streams_of[0], (SEQ, D), 1.0, 6.0, ((0, 256),))
    mixer_norm_gain = jnp.clip(1.0 + 0.18 * jax.random.normal(streams_of[1], (D,), jnp.float32), 0.1, 1.9)
    query_weight = scatter_about(streams_of[2], (D, HEADS * HEAD), D ** -0.5, 0.125, ((1, 16),))
    key_weight = scatter_about(streams_of[3], (D, HEADS * HEAD), D ** -0.5, 0.125, ((1, 16),))
    value_weight = scatter_about(streams_of[4], (D, HEADS * HEAD), D ** -0.5, 0.125, ((1, 16),))
    write_strength_projection = scatter_about(streams_of[5], (D, HEADS), D ** -0.5, 0.125)
    decay_projection = scatter_about(streams_of[6], (D, HEADS), D ** -0.5, 0.125)
    head_decay_speed = draw_head_decay_speed(jax.random.fold_in(streams_of[19], 71), 0)
    largest_write_strength = draw_largest_write_strength(jax.random.fold_in(streams_of[19], 71), 0)
    extra_log_decay = draw_extra_log_decay(jax.random.fold_in(streams_of[19], 71), 0)
    head_norm_gain = jnp.clip(1.0 + 0.18 * jax.random.normal(streams_of[10], (HEAD,), jnp.float32), 0.1, 1.9)
    mixer_output_weight = scatter_about(streams_of[11], (HEADS * HEAD, D), (HEADS * HEAD) ** -0.5, 0.125, ((0, 16),))
    expert_input_rows = scatter_about(streams_of[12], (EXP_TOKENS, D), 1.0, 6.0, ((0, 256),))
    expert_norm_gain = jnp.clip(1.0 + 0.18 * jax.random.normal(streams_of[13], (D,), jnp.float32), 0.1, 1.9)
    routes_keys = jax.random.split(jax.random.fold_in(streams_of[14], 1), EXP_TOKENS // EXP_TOK_DEV)
    routes_turns = jax.random.permutation(jax.random.fold_in(streams_of[14], 3), EXP_TOKENS // EXP_TOK_DEV)
    routes = jax.vmap(lambda own, number: routed_block(jax.random.fold_in(streams_of[14], 2), own, number, EXP_TOK_DEV, EXPERTS, TOP, CAP, 2))(routes_keys, routes_turns).reshape((EXP_TOKENS, TOP))
    expert_route_weight = jnp.clip(0.2 + 0.8 * jax.random.uniform(streams_of[15], (EXP_TOKENS, TOP), jnp.float32) ** shard_levels(streams_of[15], (EXP_TOKENS, TOP), ((0, 256),), -0.2, 0.2), 0.2, 1.0)
    gate_weight = scatter_about(streams_of[16], (EXPERTS, D, FF), D ** -0.5, 0.125, ((0, 16), (2, 16)))
    up_weight = scatter_about(streams_of[17], (EXPERTS, D, FF), D ** -0.5, 0.125, ((0, 16), (2, 16)))
    down_weight = scatter_about(streams_of[18], (EXPERTS, FF, D), FF ** -0.5, 0.0625, ((0, 16), (1, 16)))
    return {"mixer_input_rows": mixer_input_rows, "mixer_norm_gain": mixer_norm_gain, "query_weight": query_weight, "key_weight": key_weight, "value_weight": value_weight, "write_strength_projection": write_strength_projection, "decay_projection": decay_projection, "head_decay_speed": head_decay_speed, "largest_write_strength": largest_write_strength, "extra_log_decay": extra_log_decay, "head_norm_gain": head_norm_gain, "mixer_output_weight": mixer_output_weight, "expert_input_rows": expert_input_rows, "expert_norm_gain": expert_norm_gain, "routes": routes, "expert_route_weight": expert_route_weight, "gate_weight": gate_weight, "up_weight": up_weight, "down_weight": down_weight}


norm_eps = 1e-06
highest = lax.Precision.HIGHEST

def rms_scale(rows_in, gain_vec):
    widened = rows_in.astype(jnp.float32)
    scaled = widened * lax.rsqrt(lax.optimization_barrier(jnp.mean(widened * widened, axis=-1, keepdims=True)) + norm_eps)
    return (scaled * gain_vec).astype(jnp.bfloat16)

def unit_rows(tensor):
    return tensor * lax.rsqrt(lax.optimization_barrier(jnp.sum(tensor * tensor, axis=-1, keepdims=True)) + 1e-06)

def block_terms(queries, key_rows, values, log_decay_values, strength):
    length = log_decay_values.shape[-1]
    cumulative = jnp.cumsum(log_decay_values, axis=-1)
    causal = jnp.tril(jnp.ones((length, length), jnp.bool_))
    strict = jnp.tril(jnp.ones((length, length), jnp.bool_), -1)
    decays = jnp.exp(jnp.where(causal, cumulative[..., :, None] - cumulative[..., None, :], -jnp.inf))
    keys_scaled = key_rows * strength[..., None]
    inner_prod = jnp.einsum('...cd,...sd->...cs', keys_scaled, key_rows, precision=highest)
    system = jnp.where(strict, inner_prod * decays, 0.0) + jnp.eye(length, dtype=key_rows.dtype)
    right_side = jnp.concatenate([values * strength[..., None], keys_scaled * jnp.exp(cumulative)[..., None]], axis=-1)
    solved = jax.scipy.linalg.solve_triangular(system, right_side, lower=True, unit_diagonal=True)
    value_width = values.shape[-1]
    carried = solved[..., :value_width]
    weights = solved[..., value_width:]
    scores = jnp.einsum('...cd,...sd->...cs', queries, key_rows, precision=highest) * decays
    query_dec = queries * jnp.exp(cumulative)[..., None]
    keys_dec = key_rows * jnp.exp(cumulative[..., -1:] - cumulative)[..., None]
    last_decay = jnp.exp(cumulative[..., -1])
    return (carried, weights, scores, query_dec, keys_dec, last_decay)

def apply_block(memory, carried, weights, scores, query_dec, keys_dec, last_decay):
    fresh_values = carried - jnp.einsum('...cd,...de->...ce', weights, memory, precision=highest)
    output = jnp.einsum('...cd,...de->...ce', query_dec, memory, precision=highest)
    output = output + jnp.einsum('...cs,...se->...ce', scores, fresh_values, precision=highest)
    memory = memory * last_decay[..., None, None] + jnp.einsum('...cd,...ce->...de', keys_dec, fresh_values, precision=highest)
    return (memory, output)

def reference(mixer_input_rows, mixer_norm_gain, query_weight, key_weight, value_weight, write_strength_projection, decay_projection, head_decay_speed, largest_write_strength, extra_log_decay, head_norm_gain, mixer_output_weight, expert_input_rows, expert_norm_gain, routes, expert_route_weight, gate_weight, up_weight, down_weight):
    mix_normed = rms_scale(mixer_input_rows, mixer_norm_gain)

    def apply_projection(weight):
        return jnp.dot(mix_normed.astype(jnp.float32), weight.astype(jnp.float32), preferred_element_type=jnp.float32)
    queries = jax.nn.silu(apply_projection(query_weight)).reshape(SEQ, HEADS, HEAD)
    key_rows = unit_rows(jax.nn.silu(apply_projection(key_weight)).reshape(SEQ, HEADS, HEAD))
    values = jax.nn.silu(apply_projection(value_weight)).reshape(SEQ, HEADS, HEAD)
    strength = largest_write_strength * jax.nn.sigmoid(apply_projection(write_strength_projection))
    log_decay_values = extra_log_decay - head_decay_speed * jax.nn.softplus(apply_projection(decay_projection))
    block_count = SEQ // BLOCK

    def blocked(tensor):
        return tensor.reshape(block_count, BLOCK, HEADS, -1).transpose(0, 2, 1, 3)

    def advance(memory, pieces):
        return apply_block(memory, *block_terms(*pieces))
    initial = jnp.zeros((HEADS, HEAD, HEAD), jnp.float32)
    _, outputs = lax.scan(advance, initial, (blocked(queries), blocked(key_rows), blocked(values), blocked(log_decay_values[..., None])[..., 0], blocked(strength[..., None])[..., 0]))
    heads_out = outputs.transpose(0, 2, 1, 3).reshape(SEQ, HEADS, HEAD)
    head_outputs_mixed = heads_out * lax.rsqrt(lax.optimization_barrier(jnp.mean(heads_out * heads_out, axis=-1, keepdims=True)) + norm_eps)
    head_outputs_mixed = (head_outputs_mixed * head_norm_gain).reshape(SEQ, HEADS * HEAD).astype(jnp.bfloat16)
    group_width = HEADS_DEV * HEAD

    def add_group(running, group_index):
        columns = lax.dynamic_slice_in_dim(head_outputs_mixed, group_index * group_width, group_width, 1)
        weight_rows = lax.dynamic_slice_in_dim(mixer_output_weight, group_index * group_width, group_width, 0)
        partial_value = jnp.dot(columns.astype(jnp.float32), weight_rows.astype(jnp.float32), preferred_element_type=jnp.float32).astype(jnp.bfloat16)
        return (running + lax.optimization_barrier(partial_value).astype(jnp.float32), None)
    mix_total, _ = lax.scan(add_group, jnp.zeros((SEQ, D), jnp.float32), jnp.arange(N_TP, dtype=jnp.int32))
    mix_out = mix_total.astype(jnp.bfloat16)
    exp_normed = rms_scale(expert_input_rows, expert_norm_gain)
    assigned = routes.reshape(-1)
    shares = expert_route_weight.reshape(-1)
    owners = (jnp.arange(EXP_TOKENS * TOP, dtype=jnp.int32) // TOP).astype(jnp.int32)
    most_rows = N_EP * N_TP * CAP

    def expert_pass(running, expert):
        chosen = assigned == expert
        filled = jnp.sum(chosen.astype(jnp.int32))
        picked = jnp.nonzero(chosen, size=most_rows, fill_value=0)[0].astype(jnp.int32)
        live_rows = jnp.arange(most_rows, dtype=jnp.int32) < filled
        token_ids = owners[picked]
        rows_in = exp_normed[token_ids]
        gate_part = jnp.dot(rows_in.astype(jnp.float32), gate_weight[expert].astype(jnp.float32), preferred_element_type=jnp.float32)
        up_part = jnp.dot(rows_in.astype(jnp.float32), up_weight[expert].astype(jnp.float32), preferred_element_type=jnp.float32)
        hidden = (jax.nn.silu(gate_part) * up_part).astype(jnp.bfloat16)
        pieces = jnp.einsum('rgf,gfd->grd', hidden.reshape(most_rows, N_TP, FF_DEV).astype(jnp.float32), down_weight[expert].reshape(N_TP, FF_DEV, D).astype(jnp.float32))
        rounded = lax.optimization_barrier(pieces.astype(jnp.bfloat16)).astype(jnp.float32)
        expert_rows = lax.optimization_barrier(lax.optimization_barrier(jnp.sum(rounded, axis=0)).astype(jnp.bfloat16)).astype(jnp.float32)
        weight_col = jnp.where(live_rows, shares[picked], 0.0)
        return (running.at[token_ids].add(weight_col[:, None] * expert_rows), None)
    exp_total, _ = lax.scan(expert_pass, jnp.zeros((EXP_TOKENS, D), jnp.float32), jnp.arange(EXPERTS, dtype=jnp.int32))
    return (mix_out, exp_total.astype(jnp.bfloat16))
```

```python
import functools

import jax
import jax.numpy as jnp
from jax import lax
from jax.experimental import pallas as pl
from jax.experimental.pallas import tpu as pltpu
from jax.sharding import Mesh
from jax.sharding import PartitionSpec as P

HEAD = 128
BLOCK = 128
EP = ("ep_0", "ep_1")
TP = ("tp_0", "tp_1")
EP_TP = ("ep_0", "ep_1", "tp_0", "tp_1")
MESH = pl.DeviceIdType.MESH

norm_eps = 1e-06
f32 = jnp.float32
bf16 = jnp.bfloat16


def mm(a, b):
    return jnp.dot(a.astype(bf16), b.astype(bf16), preferred_element_type=f32)


def mm_nt(a, b):
    return lax.dot_general(
        a.astype(bf16), b.astype(bf16), (((1,), (1,)), ((), ())), preferred_element_type=f32
    )


def whole_of(x, axes, dim):
    for axis in reversed(axes):
        x = lax.all_gather(x, axis, axis=dim, tiled=True)
    return x


def cut_along(x, dim, devices):
    dims = x.shape
    parts = x.reshape(*dims[:dim], devices, dims[dim] // devices, *dims[dim + 1 :])
    return jnp.moveaxis(parts, dim, 0)


def sum_at_owner(x, axis, dim):
    devices = lax.axis_size(axis)
    parts = lax.all_to_all(cut_along(x, dim, devices), axis, 0, 0, tiled=True)
    return jnp.sum(parts.astype(f32), axis=0)


def rms_scale(rows_in, gain_vec):
    widened = rows_in.astype(f32)
    scaled = widened * lax.rsqrt(jnp.mean(widened * widened, axis=-1, keepdims=True) + norm_eps)
    return (scaled * gain_vec).astype(bf16)


def silu(v):
    return v / (1.0 + jnp.exp(-v))


def invert(system):
    row = lax.broadcasted_iota(jnp.int32, (BLOCK, BLOCK), 0)
    col = lax.broadcasted_iota(jnp.int32, (BLOCK, BLOCK), 1)
    apart = row ^ col
    inverse = jnp.where(row == col, 1.0, 0.0) - jnp.where(apart == 1, system, 0.0)
    size = 2
    while size < BLOCK:
        corner = jnp.where((apart >= size) & (apart < 2 * size), system, 0.0)
        rounded = inverse.astype(bf16)
        inverse = inverse - mm(mm(rounded, corner), rounded)
        size *= 2
    return inverse


def block_maps(q, k, v, strength, log_decay):
    row = lax.broadcasted_iota(jnp.int32, (BLOCK, BLOCK), 0)
    col = lax.broadcasted_iota(jnp.int32, (BLOCK, BLOCK), 1)
    lower = jnp.where(row >= col, 1.0, 0.0).astype(bf16)
    high = log_decay.astype(bf16)
    rest = log_decay - high.astype(f32)
    middle = rest.astype(bf16)
    low = (rest - middle.astype(f32)).astype(bf16)
    total = mm(lower, high) + mm(lower, middle) + mm(lower, low)
    decays = jnp.exp(jnp.where(row >= col, total - total.T, -1e30))
    both = mm_nt(jnp.concatenate([q, k], axis=0), k)
    scores = both[:BLOCK] * decays
    system = jnp.where(row > col, both[BLOCK:] * strength * decays, 0.0)
    inverse = invert(system)
    grown = jnp.exp(total)
    right = jnp.concatenate([strength * grown * k, strength * v], axis=1)
    solved = mm(inverse, right)
    last = total[BLOCK - 1 : BLOCK, :]
    keys_left = k * jnp.exp(last - total)
    joined = mm(jnp.concatenate([scores, keys_left.T], axis=0), solved)
    return (
        q * grown - joined[:BLOCK, :HEAD],
        joined[:BLOCK, HEAD:],
        joined[BLOCK:, :HEAD],
        joined[BLOCK:, HEAD:],
        jnp.exp(last),
    )


def project_pair(x, w_all, extra, speed, largest):
    p = jnp.dot(x, w_all, preferred_element_type=f32)
    q = silu(p[:, :HEAD])
    k = silu(p[:, HEAD : 2 * HEAD])
    k = k * lax.rsqrt(jnp.sum(k * k, axis=-1, keepdims=True) + 1e-06)
    v = silu(p[:, 2 * HEAD : 3 * HEAD])
    strength = largest / (1.0 + jnp.exp(-p[:, 3 * HEAD : 4 * HEAD]))
    raw = p[:, 4 * HEAD : 5 * HEAD]
    softplus = jnp.maximum(raw, 0.0) + jnp.log(1.0 + jnp.exp(-jnp.abs(raw)))
    return q, k, v, strength, extra - speed * softplus


def pair_maps(x, w_all, extra, speed, largest):
    q, k, v, strength, log_decay = project_pair(x, w_all, extra, speed, largest)
    cut = lambda a, i: a[i * BLOCK : (i + 1) * BLOCK]
    qa, oa, ga, sa, da = block_maps(*[cut(a, 0) for a in (q, k, v, strength, log_decay)])
    qb, ob, gb, sb, db = block_maps(*[cut(a, 1) for a in (q, k, v, strength, log_decay)])
    t = mm(jnp.concatenate([gb, qb], axis=0), jnp.concatenate([ga, sa], axis=1))
    g = db * ga + da * gb - t[:BLOCK, :HEAD]
    s = db * sa - t[:BLOCK, HEAD:] + sb
    qb = da * qb - t[BLOCK:, :HEAD]
    ob = t[BLOCK:, HEAD:] + ob
    return jnp.concatenate([qa, qb], axis=0), jnp.concatenate([oa, ob], axis=0), g, s, da * db


def fill_weights(w_all, wq_ref, wk_ref, wv_ref, ws_ref, wd_ref, head):
    w_all[:, 0:HEAD] = wq_ref[...]
    w_all[:, HEAD : 2 * HEAD] = wk_ref[...]
    w_all[:, 2 * HEAD : 3 * HEAD] = wv_ref[...]
    heads = ws_ref.shape[1]
    pick = jnp.where(lax.broadcasted_iota(jnp.int32, (heads, HEAD), 0) == head, 1.0, 0.0)
    w_all[:, 3 * HEAD : 4 * HEAD] = mm(ws_ref[...], pick).astype(bf16)
    w_all[:, 4 * HEAD : 5 * HEAD] = mm(wd_ref[...], pick).astype(bf16)


def span_chain(pairs, lhs_s, g_s, s_s, o_s, d_s, ps_ref, qh_ref, oh_ref):
    g = jnp.zeros((HEAD, HEAD), f32)
    s = jnp.zeros((HEAD, HEAD), f32)
    d = jnp.ones((1, HEAD), f32)
    for z in range(pairs):
        rows = pl.ds(z * 2 * BLOCK, 2 * BLOCK)
        lhs = lhs_s[z]
        t = mm(lhs, jnp.concatenate([g, s], axis=1))
        qh_ref[rows, :] = (d * lhs[HEAD:].astype(f32) - t[HEAD:, :HEAD]).astype(bf16)
        oh_ref[rows, :] = t[HEAD:, HEAD:] + o_s[z]
        dz = d_s[z, 0:1, :]
        g, s = dz * g + d * g_s[z] - t[:HEAD, :HEAD], dz * s - t[:HEAD, HEAD:] + s_s[z]
        d = d * dz
    row = lax.broadcasted_iota(jnp.int32, (HEAD, HEAD), 0)
    col = lax.broadcasted_iota(jnp.int32, (HEAD, HEAD), 1)
    ps_ref[:, :HEAD] = (jnp.where(row == col, d, 0.0) - g).astype(bf16)
    ps_ref[:, HEAD:] = s.astype(bf16)


def span_kernel(
    x_ref, wq_ref, wk_ref, wv_ref, ws_ref, wd_ref, speed_ref, largest_ref, extra_ref,
    ps_ref, qh_ref, oh_ref,
    w_all, lhs_s, g_s, s_s, o_s, d_s,
):
    head = lax.axis_index("tp_0") * 2 + lax.axis_index("tp_1")
    pairs = x_ref.shape[0] // (2 * BLOCK)
    fill_weights(w_all, wq_ref, wk_ref, wv_ref, ws_ref, wd_ref, head)

    def step(z, carry):
        rows = pl.ds(pl.multiple_of(z * 2 * BLOCK, 2 * BLOCK), 2 * BLOCK)
        q, o, g, s, d = pair_maps(
            x_ref[rows, :], w_all[...], extra_ref[rows, :], speed_ref[0], largest_ref[0]
        )
        lhs_s[z, :HEAD] = g.astype(bf16)
        lhs_s[z, HEAD:] = q.astype(bf16)
        o_s[z] = o
        g_s[z] = g
        s_s[z] = s
        d_s[z] = jnp.broadcast_to(d, (8, HEAD))
        return carry

    lax.fori_loop(0, pairs, step, 0)
    span_chain(pairs, lhs_s, g_s, s_s, o_s, d_s, ps_ref, qh_ref, oh_ref)


def span_scratch(model, pairs):
    return [
        pltpu.VMEM((model, 5 * HEAD), bf16),
        pltpu.VMEM((pairs, 3 * HEAD, HEAD), bf16),
        pltpu.VMEM((pairs, HEAD, HEAD), f32),
        pltpu.VMEM((pairs, HEAD, HEAD), f32),
        pltpu.VMEM((pairs, 2 * BLOCK, HEAD), f32),
        pltpu.VMEM((pairs, 8, HEAD), f32),
    ]


def span_call(x_rows, wq, wk, wv, ws, wd, speed, largest, extra):
    rows, model = x_rows.shape
    pairs = rows // (2 * BLOCK)
    vm = pl.BlockSpec(memory_space=pltpu.VMEM)
    sm = pl.BlockSpec(memory_space=pltpu.SMEM)
    return pl.pallas_call(
        span_kernel,
        out_shape=(
            jax.ShapeDtypeStruct((HEAD, 2 * HEAD), bf16),
            jax.ShapeDtypeStruct((rows, HEAD), bf16),
            jax.ShapeDtypeStruct((rows, HEAD), f32),
        ),
        in_specs=[vm, vm, vm, vm, vm, vm, sm, sm, vm],
        out_specs=(vm, vm, vm),
        scratch_shapes=span_scratch(model, pairs),
        compiler_params=pltpu.CompilerParams(vmem_limit_bytes=56 * 1024 * 1024),
        cost_estimate=pl.CostEstimate(
            flops=30_000_000_000, bytes_accessed=16 * 1024 * 1024, transcendentals=0
        ),
        name="span",
    )(x_rows, wq, wk, wv, ws, wd, speed, largest, extra)


def mix_kernel(
    ps_ref, qh_ref, oh_ref, gain_ref, w_ref, out_ref,
    row_maps, col_maps, total_s, heads_out, heads_in, w_s,
    w_sem, send_sem, row_sem, col_sem, head_send, head_sem,
):
    y, x = lax.axis_index("ep_0"), lax.axis_index("ep_1")
    z, c = lax.axis_index("tp_0"), lax.axis_index("tp_1")
    t = z * 2 + c
    groups = heads_in.shape[1] // HEAD
    w_copy = pltpu.make_async_copy(w_ref, w_s, w_sem)
    w_copy.start()

    barrier = pltpu.get_barrier_semaphore()
    for j in range(1, 4):
        pl.semaphore_signal(barrier, 1, device_id={"ep_1": (x + j) % 4}, device_id_type=MESH)
        pl.semaphore_signal(barrier, 1, device_id={"ep_0": (y + j) % 4}, device_id_type=MESH)
    for j in range(1, 16):
        o = (t + j) % 16
        pl.semaphore_signal(
            barrier, 1, device_id={"tp_0": o // 2, "tp_1": o % 2}, device_id_type=MESH
        )
    pl.semaphore_wait(barrier, 21)

    sends = []
    for j in range(1, 4):
        sends.append(
            pltpu.make_async_remote_copy(
                ps_ref, row_maps.at[x], send_sem.at[j], row_sem.at[x],
                device_id={"ep_1": (x + j) % 4}, device_id_type=MESH,
            )
        )
    for copy in sends:
        copy.start()
    row_maps[x] = ps_ref[...]
    for j in range(1, 4):
        o = (x + j) % 4
        pltpu.make_async_remote_copy(
            ps_ref, row_maps.at[o], send_sem.at[0], row_sem.at[o],
            device_id={"ep_1": o}, device_id_type=MESH,
        ).wait_recv()

    whole = row_maps[0]
    before = whole
    for k in range(1, 4):
        before = jnp.where(x == k, whole, before)
        later = row_maps[k]
        step = mm(later[:, :HEAD], whole)
        whole = jnp.concatenate(
            [step[:, :HEAD], step[:, HEAD:] + later[:, HEAD:].astype(f32)], axis=1
        ).astype(bf16)
    total_s[...] = whole
    sends2 = []
    for j in range(1, 4):
        sends2.append(
            pltpu.make_async_remote_copy(
                total_s, col_maps.at[y], send_sem.at[3 + j], col_sem.at[y],
                device_id={"ep_0": (y + j) % 4}, device_id_type=MESH,
            )
        )
    for copy in sends2:
        copy.start()
    col_maps[y] = whole
    for j in range(1, 4):
        o = (y + j) % 4
        pltpu.make_async_remote_copy(
            total_s, col_maps.at[o], send_sem.at[0], col_sem.at[o],
            device_id={"ep_0": o}, device_id_type=MESH,
        ).wait_recv()
    memory = jnp.zeros((HEAD, HEAD), f32)
    for k in range(3):
        earlier = col_maps[k]
        moved = earlier[:, HEAD:].astype(f32)
        if k:
            moved = moved + mm(earlier[:, :HEAD], memory)
        memory = jnp.where(k < y, moved, memory)
    moved = mm(before[:, :HEAD], memory) + before[:, HEAD:].astype(f32)
    memory = jnp.where(x > 0, moved, memory).astype(bf16)

    gain = gain_ref[...]

    def finish(n, carry):
        rows = pl.ds(pl.multiple_of(n * 2 * BLOCK, 2 * BLOCK), 2 * BLOCK)
        o = mm(qh_ref[rows, :], memory) + oh_ref[rows, :]
        o = o * lax.rsqrt(jnp.mean(o * o, axis=-1, keepdims=True) + norm_eps)
        heads_out[rows, :] = (o * gain).astype(bf16)
        return carry

    lax.fori_loop(0, groups // 2, finish, 0, unroll=True)
    mine = pl.ds(pl.multiple_of(t * HEAD, HEAD), HEAD)
    head_copies = []
    for j in range(1, 16):
        o = (t + j) % 16
        rows = pl.ds(pl.multiple_of(o * BLOCK, BLOCK), BLOCK)
        copy = pltpu.make_async_remote_copy(
            heads_out.at[rows, :], heads_in.at[:, mine], head_send.at[j], head_sem.at[t],
            device_id={"tp_0": o // 2, "tp_1": o % 2}, device_id_type=MESH,
        )
        head_copies.append(copy)
        copy.start()
    heads_in[:, mine] = heads_out[pl.ds(pl.multiple_of(t * BLOCK, BLOCK), BLOCK), :]
    for j in range(1, 16):
        o = (t + j) % 16
        cols = pl.ds(pl.multiple_of(o * HEAD, HEAD), HEAD)
        pltpu.make_async_remote_copy(
            heads_out.at[pl.ds(0, BLOCK), :], heads_in.at[:, cols], head_send.at[0], head_sem.at[o],
            device_id={"tp_0": o // 2, "tp_1": o % 2}, device_id_type=MESH,
        ).wait_recv()
    w_copy.wait()
    tile = 512

    def project(n, carry):
        cols = pl.ds(pl.multiple_of(n * tile, tile), tile)
        out_ref[:, cols] = jnp.dot(
            heads_in[...], w_s[:, cols], preferred_element_type=f32
        ).astype(bf16)
        return carry

    lax.fori_loop(0, out_ref.shape[1] // tile, project, 0)
    for copy in sends + sends2 + head_copies:
        copy.wait_send()


def mix_call(ps, qh, oh, gain, w_whole):
    rows = qh.shape[0]
    model = w_whole.shape[1]
    vm = pl.BlockSpec(memory_space=pltpu.VMEM)
    return pl.pallas_call(
        mix_kernel,
        out_shape=jax.ShapeDtypeStruct((BLOCK, model), bf16),
        in_specs=[vm, vm, vm, vm, pl.BlockSpec(memory_space=pl.ANY)],
        out_specs=vm,
        scratch_shapes=[
            pltpu.VMEM((4, HEAD, 2 * HEAD), bf16),
            pltpu.VMEM((4, HEAD, 2 * HEAD), bf16),
            pltpu.VMEM((HEAD, 2 * HEAD), bf16),
            pltpu.VMEM((rows, HEAD), bf16),
            pltpu.VMEM((BLOCK, w_whole.shape[0]), bf16),
            pltpu.VMEM(w_whole.shape, bf16),
            pltpu.SemaphoreType.DMA,
            pltpu.SemaphoreType.DMA((7,)),
            pltpu.SemaphoreType.DMA((4,)),
            pltpu.SemaphoreType.DMA((4,)),
            pltpu.SemaphoreType.DMA((16,)),
            pltpu.SemaphoreType.DMA((16,)),
        ],
        compiler_params=pltpu.CompilerParams(
            vmem_limit_bytes=48 * 1024 * 1024, collective_id=1, has_side_effects=True
        ),
        cost_estimate=pl.CostEstimate(
            flops=10_000_000_000, bytes_accessed=16 * 1024 * 1024, transcendentals=0
        ),
        name="mix",
    )(ps, qh, oh, gain, w_whole)


def expert_hidden(rows_in, gate_weight, up_weight):
    gate_part = jnp.dot(rows_in, gate_weight[0], preferred_element_type=f32)
    up_part = jnp.dot(rows_in, up_weight[0], preferred_element_type=f32)
    return (jax.nn.silu(gate_part) * up_part).astype(bf16)


def slot_numbers(routes, experts, capacity):
    assigned = routes.reshape(-1)
    onehot = (assigned[:, None] == jnp.arange(experts, dtype=jnp.int32)[None, :]).astype(jnp.int32)
    before = jnp.cumsum(onehot, axis=0) - onehot
    return assigned * capacity + jnp.sum(before * onehot, axis=1)


def body(
    mixer_input_rows,
    mixer_norm_gain,
    query_weight,
    key_weight,
    value_weight,
    write_strength_projection,
    decay_projection,
    head_decay_speed,
    largest_write_strength,
    extra_log_decay,
    head_norm_gain,
    mixer_output_weight,
    expert_input_rows,
    expert_norm_gain,
    routes,
    expert_route_weight,
    gate_weight,
    up_weight,
    down_weight,
):
    w_whole = lax.all_gather(mixer_output_weight, TP, axis=0, tiled=True)
    mix_normed = rms_scale(mixer_input_rows, mixer_norm_gain)
    exp_normed = rms_scale(expert_input_rows, expert_norm_gain)
    token_count, top_count = routes.shape
    model_width = exp_normed.shape[1]
    experts = gate_weight.shape[0] * lax.axis_size(EP)
    capacity = 2
    slot_ids = slot_numbers(routes, experts, capacity)
    places = jnp.arange(experts * capacity, dtype=jnp.int32)
    selector = jnp.sum(
        (slot_ids.reshape(token_count, top_count)[None, :, :] == places[:, None, None]).astype(f32),
        axis=2,
    )
    sending = jnp.dot(
        selector.astype(bf16), exp_normed, preferred_element_type=f32
    ).astype(bf16)
    arrived = lax.all_to_all(
        sending.reshape(experts, capacity, model_width), EP, split_axis=0, concat_axis=0, tiled=True
    )
    arrived = arrived.reshape(-1, model_width)
    ps, qh, oh = span_call(
        lax.all_gather(mix_normed, TP, axis=0, tiled=True),
        query_weight, key_weight, value_weight,
        write_strength_projection, decay_projection,
        head_decay_speed, largest_write_strength, extra_log_decay,
    )
    mix_out = mix_call(ps, qh, oh, head_norm_gain.reshape(1, HEAD), w_whole)
    hidden = expert_hidden(whole_of(arrived, TP, 0), gate_weight, up_weight)
    expert_sum = sum_at_owner(
        jnp.dot(hidden, down_weight[0], preferred_element_type=f32).astype(bf16),
        TP,
        0,
    )
    finished = expert_sum.astype(bf16).reshape(experts, capacity, model_width)
    returned = lax.all_to_all(finished, EP, split_axis=0, concat_axis=0, tiled=True)
    results = returned.reshape(experts * capacity, model_width)[slot_ids].astype(f32)
    results = results.reshape(token_count, top_count, model_width)
    exp_out = jnp.sum(results * expert_route_weight[:, :, None], axis=1).astype(bf16)
    return (mix_out, exp_out)


def solution(mesh):
    torus = Mesh(mesh.devices.reshape(4, 4, 8, 2), ("ep_0", "ep_1", "tp_0", "tp_1"))
    placed = (
        P(EP_TP, None),
        P(),
        P(None, TP),
        P(None, TP),
        P(None, TP),
        P(),
        P(),
        P(TP),
        P(TP),
        P(EP, TP),
        P(),
        P(TP, None),
        P(EP_TP, None),
        P(),
        P(EP_TP, None),
        P(EP_TP, None),
        P(EP, None, TP),
        P(EP, None, TP),
        P(EP, TP, None),
    )
    return jax.shard_map(
        body,
        mesh=torus,
        in_specs=placed,
        out_specs=(P(EP_TP, None), P(EP_TP, None)),
        check_vma=False,
    )
```

```python
import functools

import jax
import jax.numpy as jnp
from jax import lax
from jax.experimental import pallas as pl
from jax.experimental.pallas import tpu as pltpu
from jax.sharding import Mesh
from jax.sharding import PartitionSpec as P

HEAD = 128
BLOCK = 128
EP = ("ep_0", "ep_1")
TP = ("tp_0", "tp_1")
EP_TP = ("ep_0", "ep_1", "tp_0", "tp_1")
MESH = pl.DeviceIdType.MESH

norm_eps = 1e-06
f32 = jnp.float32
bf16 = jnp.bfloat16


def mm(a, b):
    return jnp.dot(a.astype(bf16), b.astype(bf16), preferred_element_type=f32)


def mm_nt(a, b):
    return lax.dot_general(
        a.astype(bf16), b.astype(bf16), (((1,), (1,)), ((), ())), preferred_element_type=f32
    )


def silu(v):
    return v / (1.0 + jnp.exp(-v))


def project_pair(x, w_all, extra, speed, largest):
    p = jnp.dot(x, w_all, preferred_element_type=f32)
    q = silu(p[:, :HEAD])
    k = silu(p[:, HEAD : 2 * HEAD])
    k = k * lax.rsqrt(jnp.sum(k * k, axis=-1, keepdims=True) + 1e-06)
    v = silu(p[:, 2 * HEAD : 3 * HEAD])
    strength = largest / (1.0 + jnp.exp(-p[:, 3 * HEAD : 4 * HEAD]))
    raw = p[:, 4 * HEAD : 5 * HEAD]
    softplus = jnp.maximum(raw, 0.0) + jnp.log(1.0 + jnp.exp(-jnp.abs(raw)))
    return q, k, v, strength, extra - speed * softplus


def lockstep_invert(systems):
    row = lax.broadcasted_iota(jnp.int32, (BLOCK, BLOCK), 0)
    col = lax.broadcasted_iota(jnp.int32, (BLOCK, BLOCK), 1)
    apart = row ^ col
    eye = jnp.where(row == col, 1.0, 0.0)
    inverses = [eye - jnp.where(apart == 1, a, 0.0) for a in systems]
    size = 2
    while size < BLOCK:
        keep = (apart >= size) & (apart < 4 * size)
        xs = [a.astype(bf16) for a in inverses]
        ns = [mm(x, jnp.where(keep, a, 0.0)).astype(bf16) for x, a in zip(xs, systems)]
        ys = [a - mm(n, x) for a, n, x in zip(inverses, ns, xs)]
        squares = [mm(n, n) for n in ns]
        inverses = [y + mm(n2, y) for y, n2 in zip(ys, squares)]
        size *= 4
    return inverses


def block_maps(qs, ks, vs, strengths, log_decays):
    row = lax.broadcasted_iota(jnp.int32, (BLOCK, BLOCK), 0)
    col = lax.broadcasted_iota(jnp.int32, (BLOCK, BLOCK), 1)
    lower = jnp.where(row >= col, 1.0, 0.0).astype(bf16)
    parts = []
    for a in log_decays:
        high = a.astype(bf16)
        rest = a - high.astype(f32)
        middle = rest.astype(bf16)
        parts.append((high, middle, (rest - middle.astype(f32)).astype(bf16)))
    totals = [mm(lower, h) + mm(lower, m) + mm(lower, l) for h, m, l in parts]
    boths = [mm_nt(jnp.concatenate([q, k], axis=0), k) for q, k in zip(qs, ks)]
    decays = [jnp.exp(jnp.where(row >= col, a - a.T, -1e30)) for a in totals]
    scores = [b[:BLOCK] * d for b, d in zip(boths, decays)]
    systems = [
        jnp.where(row > col, b[BLOCK:] * s * d, 0.0) for b, s, d in zip(boths, strengths, decays)
    ]
    inverses = lockstep_invert(systems)
    growns = [jnp.exp(a) for a in totals]
    rights = [
        jnp.concatenate([s * g * k, s * v], axis=1)
        for s, g, k, v in zip(strengths, growns, ks, vs)
    ]
    solveds = [mm(a, b) for a, b in zip(inverses, rights)]
    lasts = [a[BLOCK - 1 : BLOCK, :] for a in totals]
    lefts = [
        jnp.concatenate([s, (k * jnp.exp(last - a)).T], axis=0)
        for s, k, last, a in zip(scores, ks, lasts, totals)
    ]
    joineds = [mm(a, b) for a, b in zip(lefts, solveds)]
    return [
        (q * g - j[:BLOCK, :HEAD], j[:BLOCK, HEAD:], j[BLOCK:, :HEAD], j[BLOCK:, HEAD:], jnp.exp(last))
        for q, g, j, last in zip(qs, growns, joineds, lasts)
    ]


def pairs_maps(xs, w_all, extras, speed, largest):
    columns = [[], [], [], [], []]
    for x, extra in zip(xs, extras):
        for list_, a in zip(columns, project_pair(x, w_all, extra, speed, largest)):
            list_ += [a[:BLOCK], a[BLOCK:]]
    blocks = block_maps(*columns)
    results = []
    for a, b in zip(blocks[0::2], blocks[1::2]):
        (qa, oa, ga, sa, da), (qb, ob, gb, sb, db) = a, b
        t = mm(jnp.concatenate([gb, qb], axis=0), jnp.concatenate([ga, sa], axis=1))
        g = db * ga + da * gb - t[:BLOCK, :HEAD]
        s = db * sa - t[:BLOCK, HEAD:] + sb
        qb = da * qb - t[BLOCK:, :HEAD]
        ob = t[BLOCK:, HEAD:] + ob
        results.append(
            (jnp.concatenate([qa, qb], axis=0), jnp.concatenate([oa, ob], axis=0), g, s, da * db)
        )
    return results


CHIPS = 8
RING = 4
EPS = RING * RING
SLOTS = 2
ROWS = EPS * SLOTS
MSG = 8


def normed(x, gain):
    widened = x.astype(f32)
    scaled = widened * lax.rsqrt(jnp.mean(widened * widened, axis=-1, keepdims=True) + norm_eps)
    return (scaled * gain).astype(bf16)


def three_parts(a):
    high = a.astype(bf16)
    rest = a - high.astype(f32)
    middle = rest.astype(bf16)
    return high, middle, (rest - middle.astype(f32)).astype(bf16)


def layer_kernel(
    xm_ref, mgain_ref, xe_ref, egain_ref, routes_ref, share_ref, extra_ref, speed_ref, largest_ref,
    hgain_ref, wst_ref, wdt_ref, wq_ref, wk_ref, wv_ref, wo_ref, gate_ref, up_ref, down_ref,
    mix_ref, exp_ref,
    w_all, gate_s, up_s, down_s, xb, eb, lhs_s, g_s, s_s, o_s, d_s, ps_s, qh_s, oh_s,
    row_maps, col_maps, total_s, heads_out, heads_in, wg,
    msg_out, msg_in, pb, pr, ss, rl, ret_out, ret_in,
    load_sem, ring_send, ring_recv, msg_send, msg_recv, ret_send, ret_recv, w_send, w_recv,
    pb_send, pb_recv, rs_send, rs_recv, map_send, row_recv, col_recv, head_send, head_recv,
):
    y, x = lax.axis_index("ep_0"), lax.axis_index("ep_1")
    z, c = lax.axis_index("tp_0"), lax.axis_index("tp_1")
    e = y * RING + x
    t = z * 2 + c
    other = 1 - c

    def at_tp(chip, core):
        return {"tp_0": chip, "tp_1": core}

    def at_ep(o):
        return {"ep_0": o // RING, "ep_1": o % RING}

    def remote(src, dst, send, recv, where):
        return pltpu.make_async_remote_copy(
            src, dst, send, recv, device_id=where, device_id_type=MESH
        )

    loads = [
        pltpu.make_async_copy(wq_ref, w_all.at[:, pl.ds(0, HEAD)], load_sem.at[0]),
        pltpu.make_async_copy(wk_ref, w_all.at[:, pl.ds(HEAD, HEAD)], load_sem.at[1]),
        pltpu.make_async_copy(wv_ref, w_all.at[:, pl.ds(2 * HEAD, HEAD)], load_sem.at[2]),
        pltpu.make_async_copy(gate_ref.at[0], gate_s, load_sem.at[3]),
        pltpu.make_async_copy(up_ref.at[0], up_s, load_sem.at[4]),
        pltpu.make_async_copy(down_ref.at[0], down_s, load_sem.at[5]),
        pltpu.make_async_copy(
            wo_ref.at[:, pl.ds(pl.multiple_of(e * HEAD, HEAD), HEAD)], wg.at[c, e, z], load_sem.at[6]
        ),
    ]
    for copy in loads:
        copy.start()

    barrier = pltpu.get_barrier_semaphore()
    for j in range(1, 16):
        o = (t + j) % 16
        pl.semaphore_signal(barrier, 1, device_id=at_tp(o // 2, o % 2), device_id_type=MESH)
        pl.semaphore_signal(barrier, 1, device_id=at_ep((e + j) % EPS), device_id_type=MESH)

    xb[t] = normed(xm_ref[...], mgain_ref[...])

    lane = lax.broadcasted_iota(jnp.int32, (MSG, 128), 1)
    first = jnp.where(lane // MSG == routes_ref[:, 0:1], 1.0, 0.0)
    second = jnp.where(lane // MSG == routes_ref[:, 1:2], 1.0, 0.0)
    named = first + second
    before = jnp.zeros((MSG, 128), f32)
    token = lax.broadcasted_iota(jnp.int32, (MSG, 128), 0)
    for i in range(MSG - 1):
        before = before + jnp.where(token > i, named[i : i + 1, :], 0.0)
    fills = jnp.where(before == (lane % MSG).astype(f32), named, 0.0)
    shares = fills * (first * share_ref[:, 0:1] + second * share_ref[:, 1:2])
    xn = normed(xe_ref[...], egain_ref[...])
    messages = mm(fills.T, xn)
    for o in range(EPS):
        msg_out[o] = messages[o * MSG : (o + 1) * MSG].astype(bf16)
    pl.semaphore_wait(barrier, 30)

    def ring_copy(block, part, way, where):
        buffer = xb if part == 0 else eb
        return remote(
            buffer.at[block], buffer.at[block], ring_send.at[block, part, way],
            ring_recv.at[block, part], where,
        )

    up_chip, down_chip = (z + 1) % CHIPS, (z + CHIPS - 1) % CHIPS

    def send_own(part):
        ring_copy(t, part, 0, at_tp(up_chip, c)).start()
        ring_copy(t, part, 1, at_tp(down_chip, c)).start()
        ring_copy(t, part, 2, at_tp(z, other)).start()

    def arrived(block, part):
        ring_copy(block, part, 0, at_tp(up_chip, c)).wait_recv()

    send_own(0)
    msg_copies = []
    for j in range(1, EPS):
        o = (e + j) % EPS
        msg_copies.append(
            remote(msg_out.at[o], msg_in.at[e], msg_send.at[j], msg_recv.at[e], at_ep(o))
        )
    for copy in msg_copies:
        copy.start()
    msg_in[e] = msg_out[e]

    heads = wst_ref.shape[0]
    pick = jnp.where(lax.broadcasted_iota(jnp.int32, (heads, HEAD), 0) == t, 1.0, 0.0)
    w_all[:, 3 * HEAD : 4 * HEAD] = mm(wst_ref[...].astype(f32).T, pick).astype(bf16)
    w_all[:, 4 * HEAD : 5 * HEAD] = mm(wdt_ref[...].astype(f32).T, pick).astype(bf16)

    loads[6].wait()
    w_copies = []
    for j in range(1, CHIPS):
        o = (z + j) % CHIPS
        w_copies.append(
            remote(wg.at[c, e, z], wg.at[c, e, z], w_send.at[j], w_recv.at[z], at_tp(o, c))
        )
    for copy in w_copies:
        copy.start()

    for j in range(1, EPS):
        o = (e + j) % EPS
        remote(msg_out.at[0], msg_in.at[o], msg_send.at[0], msg_recv.at[o], at_ep(o)).wait_recv()
    landed = jnp.concatenate([msg_in[o].astype(f32) for o in range(EPS)], axis=0)
    slot = lax.broadcasted_iota(jnp.int32, (ROWS, EPS * MSG), 0)
    line = lax.broadcasted_iota(jnp.int32, (ROWS, EPS * MSG), 1)
    squeeze = jnp.where(
        (line // MSG == slot // SLOTS) & (line % MSG == slot % SLOTS), 1.0, 0.0
    )
    eb[t] = mm(squeeze, landed).astype(bf16)
    for copy in loads[:3]:
        copy.wait()
    send_own(1)

    speed, largest = speed_ref[0], largest_ref[0]

    def extra_of(chip):
        rows = [
            jnp.broadcast_to(extra_ref[chip * 2 + i], (HEAD, BLOCK)).T for i in range(2)
        ]
        return jnp.concatenate(rows, axis=0)

    def span_group(chips):
        xs = [jnp.concatenate([xb[chip * 2], xb[chip * 2 + 1]], axis=0) for chip in chips]
        extras = [extra_of(chip) for chip in chips]
        for chip, (q, o, g, s, d) in zip(chips, pairs_maps(xs, w_all[...], extras, speed, largest)):
            lhs_s[chip, :HEAD] = g.astype(bf16)
            lhs_s[chip, HEAD:] = q.astype(bf16)
            o_s[chip] = o
            g_s[chip] = g
            s_s[chip] = s
            d_s[chip] = jnp.broadcast_to(d, (8, HEAD))

    def pb_copy(chip):
        return remote(
            pb.at[chip, other], pr.at[chip], pb_send.at[chip], pb_recv.at[chip], at_tp(z, other)
        )

    def expert_group(chips):
        rows = jnp.concatenate(
            [eb[chip * 2 + i] for chip in chips for i in range(2)], axis=0
        )
        gated = jnp.dot(rows, gate_s[...], preferred_element_type=f32)
        raised = jnp.dot(rows, up_s[...], preferred_element_type=f32)
        hidden = (silu(gated) * raised).astype(bf16)
        width = 1024
        for n in range(0, down_s.shape[1], width):
            part = jnp.dot(hidden, down_s[:, n : n + width], preferred_element_type=f32)
            for i, chip in enumerate(chips):
                for core in range(2):
                    start = (i * 2 + core) * ROWS
                    pb[chip, core, :, n : n + width] = part[start : start + ROWS].astype(bf16)
        for chip in chips:
            pb_copy(chip).start()

    def rs_copy(chip):
        return remote(ss.at[chip], rl.at[z], rs_send.at[chip], rs_recv.at[z], at_tp(chip, c))

    def add_partner(chip):
        pb_copy(chip).wait_recv()
        ss[chip] = (pb[chip, c].astype(f32) + pr[chip].astype(f32)).astype(bf16)

    arrived(z * 2 + other, 0)
    span_group([z])
    for copy in loads[3:6]:
        copy.wait()
    arrived(z * 2 + other, 1)
    expert_group([z])

    for j in range(1, CHIPS):
        o = (z + j) % CHIPS
        remote(wg.at[c, e, o], wg.at[c, e, o], w_send.at[0], w_recv.at[o], at_tp(o, c)).wait_recv()
    wx_copies = []
    for j in range(1, RING):
        wx_copies.append(
            remote(
                wg.at[c, e], wg.at[c, e], w_send.at[CHIPS + j], w_recv.at[CHIPS + x],
                {"ep_1": (x + j) % RING},
            )
        )
    for copy in wx_copies:
        copy.start()

    def step(k, carry):
        behind, ahead = (z + CHIPS - k) % CHIPS, (z + k) % CHIPS

        def forward(part):
            @pl.when((k < 3) | (c == 0))
            def _():
                ring_copy(behind * 2 + c, part, 0, at_tp(up_chip, c)).start()

            @pl.when((k < 3) | (c == 1))
            def _():
                ring_copy(ahead * 2 + c, part, 1, at_tp(down_chip, c)).start()

        for part in range(2):
            arrived(behind * 2 + c, part)
            arrived(ahead * 2 + c, part)
            forward(part)
            ring_copy(behind * 2 + c, part, 2, at_tp(z, other)).start()
            ring_copy(ahead * 2 + c, part, 2, at_tp(z, other)).start()
            arrived(behind * 2 + other, part)
            arrived(ahead * 2 + other, part)
            if part == 0:
                span_group([behind, ahead])
            else:
                expert_group([behind, ahead])
        return carry

    lax.fori_loop(1, 3, step, 0)
    for j in range(1, RING):
        o = (x + j) % RING
        remote(
            wg.at[c, y * RING + o], wg.at[c, y * RING + o], w_send.at[0], w_recv.at[CHIPS + o],
            {"ep_1": o},
        ).wait_recv()
    wy_copies = []
    for j in range(1, RING):
        line_of = wg.at[c, pl.ds(y * RING, RING)]
        wy_copies.append(
            remote(
                line_of, line_of, w_send.at[CHIPS + RING + j], w_recv.at[CHIPS + RING + y],
                {"ep_0": (y + j) % RING},
            )
        )
    for copy in wy_copies:
        copy.start()
    lax.fori_loop(3, 4, step, 0)

    far = (z + 4) % CHIPS
    for j in range(CHIPS):
        if j != 4:
            chip = (z + j) % CHIPS
            add_partner(chip)
            if j:
                rs_copy(chip).start()
    arrived(far * 2 + c, 0)
    ring_copy(far * 2 + c, 0, 2, at_tp(z, other)).start()
    arrived(far * 2 + other, 0)
    span_group([far])

    g = jnp.zeros((HEAD, HEAD), f32)
    s = jnp.zeros((HEAD, HEAD), f32)
    d = jnp.ones((1, HEAD), f32)
    for chip in range(CHIPS):
        rows = slice(chip * 2 * BLOCK, (chip + 1) * 2 * BLOCK)
        lhs = lhs_s[chip]
        m = mm(lhs, jnp.concatenate([g, s], axis=1))
        qh_s[rows, :] = (d * lhs[HEAD:].astype(f32) - m[HEAD:, :HEAD]).astype(bf16)
        oh_s[rows, :] = m[HEAD:, HEAD:] + o_s[chip]
        dz = d_s[chip, 0:1, :]
        g, s = dz * g + d * g_s[chip] - m[:HEAD, :HEAD], dz * s - m[:HEAD, HEAD:] + s_s[chip]
        d = d * dz
    row = lax.broadcasted_iota(jnp.int32, (HEAD, HEAD), 0)
    col = lax.broadcasted_iota(jnp.int32, (HEAD, HEAD), 1)
    own_map = jnp.concatenate([jnp.where(row == col, d, 0.0) - g, s], axis=1).astype(bf16)
    ps_s[...] = own_map
    map_copies = []
    for j in range(1, RING):
        map_copies.append(
            remote(
                ps_s, row_maps.at[x], map_send.at[j], row_recv.at[x], {"ep_1": (x + j) % RING}
            )
        )
    for copy in map_copies:
        copy.start()
    row_maps[x] = own_map

    arrived(far * 2 + c, 1)
    ring_copy(far * 2 + c, 1, 2, at_tp(z, other)).start()
    arrived(far * 2 + other, 1)
    expert_group([far])

    for j in range(1, RING):
        o = (x + j) % RING
        remote(ps_s, row_maps.at[o], map_send.at[0], row_recv.at[o], {"ep_1": o}).wait_recv()
    whole = row_maps[0]
    mine = whole
    for k in range(1, RING):
        mine = jnp.where(x == k, whole, mine)
        later = row_maps[k]
        m = mm(later[:, :HEAD], whole)
        whole = jnp.concatenate(
            [m[:, :HEAD], m[:, HEAD:] + later[:, HEAD:].astype(f32)], axis=1
        ).astype(bf16)
    total_s[...] = whole
    total_copies = []
    for j in range(1, RING):
        total_copies.append(
            remote(
                total_s, col_maps.at[y], map_send.at[RING + j], col_recv.at[y],
                {"ep_0": (y + j) % RING},
            )
        )
    for copy in total_copies:
        copy.start()
    col_maps[y] = whole

    add_partner(far)
    rs_copy(far).start()
    for j in range(1, RING):
        o = (y + j) % RING
        line_of = wg.at[c, pl.ds(o * RING, RING)]
        remote(
            line_of, line_of, w_send.at[0], w_recv.at[CHIPS + RING + o], {"ep_0": o}
        ).wait_recv()
    w_half = remote(
        wg.at[c], wg.at[c], w_send.at[CHIPS + 2 * RING], w_recv.at[CHIPS + 2 * RING],
        at_tp(z, other),
    )
    w_half.start()

    for j in range(1, RING):
        o = (y + j) % RING
        remote(
            total_s, col_maps.at[o], map_send.at[0], col_recv.at[o], {"ep_0": o}
        ).wait_recv()
    memory = jnp.zeros((HEAD, HEAD), f32)
    for k in range(RING - 1):
        earlier = col_maps[k]
        moved = earlier[:, HEAD:].astype(f32)
        if k:
            moved = moved + mm(earlier[:, :HEAD], memory)
        memory = jnp.where(k < y, moved, memory)
    moved = mm(mine[:, :HEAD], memory) + mine[:, HEAD:].astype(f32)
    memory = jnp.where(x > 0, moved, memory).astype(bf16)

    hgain = hgain_ref[...]
    for chip in range(CHIPS):
        rows = slice(chip * 2 * BLOCK, (chip + 1) * 2 * BLOCK)
        o = mm(qh_s[rows, :], memory) + oh_s[rows, :]
        o = o * lax.rsqrt(jnp.mean(o * o, axis=-1, keepdims=True) + norm_eps)
        heads_out[rows, :] = (o * hgain).astype(bf16)
    own_cols = pl.ds(pl.multiple_of(t * HEAD, HEAD), HEAD)
    head_copies = []
    for j in range(1, 16):
        o = (t + j) % 16
        rows = pl.ds(pl.multiple_of(o * BLOCK, BLOCK), BLOCK)
        head_copies.append(
            remote(
                heads_out.at[rows, :], heads_in.at[:, own_cols], head_send.at[j], head_recv.at[t],
                at_tp(o // 2, o % 2),
            )
        )
    for copy in head_copies:
        copy.start()
    heads_in[:, own_cols] = heads_out[pl.ds(pl.multiple_of(t * BLOCK, BLOCK), BLOCK), :]

    total = ss[z].astype(f32)
    for j in range(1, CHIPS):
        o = (z + j) % CHIPS
        remote(ss.at[0], rl.at[o], rs_send.at[o], rs_recv.at[o], at_tp(o, c)).wait_recv()
        total = total + rl[o].astype(f32)
    spread_line = lax.broadcasted_iota(jnp.int32, (EPS * MSG, ROWS), 0)
    spread_slot = lax.broadcasted_iota(jnp.int32, (EPS * MSG, ROWS), 1)
    spread = jnp.where(
        (spread_line // MSG == spread_slot // SLOTS)
        & (spread_line % MSG == spread_slot % SLOTS),
        1.0,
        0.0,
    )
    returning = mm(spread, total)
    for o in range(EPS):
        ret_out[o] = returning[o * MSG : (o + 1) * MSG].astype(bf16)
    ret_copies = []
    for j in range(1, EPS):
        o = (e + j) % EPS
        ret_copies.append(
            remote(ret_out.at[o], ret_in.at[e], ret_send.at[j], ret_recv.at[e], at_ep(o))
        )
    for copy in ret_copies:
        copy.start()
    ret_in[e] = ret_out[e]

    remote(
        wg.at[other], wg.at[other], w_send.at[0], w_recv.at[CHIPS + 2 * RING], at_tp(z, other)
    ).wait_recv()
    for j in range(1, 16):
        o = (t + j) % 16
        cols = pl.ds(pl.multiple_of(o * HEAD, HEAD), HEAD)
        remote(
            heads_out.at[pl.ds(0, BLOCK), :], heads_in.at[:, cols], head_send.at[0],
            head_recv.at[o], at_tp(o // 2, o % 2),
        ).wait_recv()
    for pair in range(EPS // 2):
        weight = jnp.concatenate(
            [
                jnp.concatenate(
                    [wg[core, 2 * pair + i, chip] for chip in range(CHIPS) for core in range(2)],
                    axis=0,
                )
                for i in range(2)
            ],
            axis=1,
        )
        mix_ref[:, pair * 2 * HEAD : (pair + 1) * 2 * HEAD] = jnp.dot(
            heads_in[...], weight, preferred_element_type=f32
        ).astype(bf16)

    for j in range(1, EPS):
        o = (e + j) % EPS
        remote(ret_out.at[0], ret_in.at[o], ret_send.at[0], ret_recv.at[o], at_ep(o)).wait_recv()
    results = jnp.concatenate([ret_in[o].astype(f32) for o in range(EPS)], axis=0).astype(bf16)
    out = sum(jnp.dot(a, results, preferred_element_type=f32) for a in three_parts(shares))
    exp_ref[...] = out.astype(bf16)

    for copy in (
        msg_copies + w_copies + wx_copies + wy_copies + [w_half] + map_copies + total_copies
        + head_copies + ret_copies
    ):
        copy.wait_send()
    for part in range(2):
        ring_copy(t, part, 0, at_tp(up_chip, c)).wait_send()
        ring_copy(t, part, 1, at_tp(down_chip, c)).wait_send()
        ring_copy(t, part, 2, at_tp(z, other)).wait_send()
        for k in range(1, 4):
            behind, ahead = (z + CHIPS - k) % CHIPS, (z + k) % CHIPS

            @pl.when((k < 3) | (c == 0))
            def _():
                ring_copy(behind * 2 + c, part, 0, at_tp(up_chip, c)).wait_send()

            @pl.when((k < 3) | (c == 1))
            def _():
                ring_copy(ahead * 2 + c, part, 1, at_tp(down_chip, c)).wait_send()

            ring_copy(behind * 2 + c, part, 2, at_tp(z, other)).wait_send()
            ring_copy(ahead * 2 + c, part, 2, at_tp(z, other)).wait_send()
        ring_copy(far * 2 + c, part, 2, at_tp(z, other)).wait_send()
    for chip in range(CHIPS):
        pb_copy(chip).wait_send()
    for j in range(1, CHIPS):
        rs_copy((z + j) % CHIPS).wait_send()


def body(
    mixer_input_rows,
    mixer_norm_gain,
    query_weight,
    key_weight,
    value_weight,
    write_strength_projection,
    decay_projection,
    head_decay_speed,
    largest_write_strength,
    extra_log_decay,
    head_norm_gain,
    mixer_output_weight,
    expert_input_rows,
    expert_norm_gain,
    routes,
    expert_route_weight,
    gate_weight,
    up_weight,
    down_weight,
):
    rows, model = mixer_input_rows.shape
    tokens = expert_input_rows.shape[0]
    hidden = gate_weight.shape[2]
    span = extra_log_decay.shape[0]
    blocks = span // BLOCK
    vm = pl.BlockSpec(memory_space=pltpu.VMEM)
    sm = pl.BlockSpec(memory_space=pltpu.SMEM)
    hbm = pl.BlockSpec(memory_space=pl.ANY)
    dma = pltpu.SemaphoreType.DMA
    return pl.pallas_call(
        layer_kernel,
        out_shape=(
            jax.ShapeDtypeStruct((rows, model), bf16),
            jax.ShapeDtypeStruct((tokens, model), bf16),
        ),
        in_specs=[vm] * 7 + [sm] * 2 + [vm] * 3 + [hbm] * 7,
        out_specs=(vm, vm),
        scratch_shapes=[
            pltpu.VMEM((model, 5 * HEAD), bf16),
            pltpu.VMEM((model, hidden), bf16),
            pltpu.VMEM((model, hidden), bf16),
            pltpu.VMEM((hidden, model), bf16),
            pltpu.VMEM((blocks, BLOCK, model), bf16),
            pltpu.VMEM((blocks, ROWS, model), bf16),
            pltpu.VMEM((CHIPS, 3 * HEAD, HEAD), bf16),
            pltpu.VMEM((CHIPS, HEAD, HEAD), f32),
            pltpu.VMEM((CHIPS, HEAD, HEAD), f32),
            pltpu.VMEM((CHIPS, 2 * BLOCK, HEAD), f32),
            pltpu.VMEM((CHIPS, 8, HEAD), f32),
            pltpu.VMEM((HEAD, 2 * HEAD), bf16),
            pltpu.VMEM((span, HEAD), bf16),
            pltpu.VMEM((span, HEAD), f32),
            pltpu.VMEM((RING, HEAD, 2 * HEAD), bf16),
            pltpu.VMEM((RING, HEAD, 2 * HEAD), bf16),
            pltpu.VMEM((HEAD, 2 * HEAD), bf16),
            pltpu.VMEM((span, HEAD), bf16),
            pltpu.VMEM((BLOCK, model), bf16),
            pltpu.VMEM((2, EPS, CHIPS, HEAD, HEAD), bf16),
            pltpu.VMEM((EPS, MSG, model), bf16),
            pltpu.VMEM((EPS, MSG, model), bf16),
            pltpu.VMEM((CHIPS, 2, ROWS, model), bf16),
            pltpu.VMEM((CHIPS, ROWS, model), bf16),
            pltpu.VMEM((CHIPS, ROWS, model), bf16),
            pltpu.VMEM((CHIPS, ROWS, model), bf16),
            pltpu.VMEM((EPS, MSG, model), bf16),
            pltpu.VMEM((EPS, MSG, model), bf16),
            dma((7,)),
            dma((16, 2, 3)),
            dma((16, 2)),
            dma((EPS,)),
            dma((EPS,)),
            dma((EPS,)),
            dma((EPS,)),
            dma((CHIPS + 2 * RING + 1,)),
            dma((CHIPS + 2 * RING + 1,)),
            dma((CHIPS,)),
            dma((CHIPS,)),
            dma((CHIPS,)),
            dma((CHIPS,)),
            dma((2 * RING,)),
            dma((RING,)),
            dma((RING,)),
            dma((16,)),
            dma((16,)),
        ],
        compiler_params=pltpu.CompilerParams(
            vmem_limit_bytes=60 * 1024 * 1024, collective_id=1, has_side_effects=True
        ),
        cost_estimate=pl.CostEstimate(
            flops=10_000_000_000, bytes_accessed=32 * 1024 * 1024, transcendentals=0
        ),
        name="layer",
    )(
        mixer_input_rows, mixer_norm_gain.reshape(1, model), expert_input_rows,
        expert_norm_gain.reshape(1, model), routes, expert_route_weight,
        extra_log_decay.reshape(blocks, 1, BLOCK), head_decay_speed, largest_write_strength,
        head_norm_gain.reshape(1, HEAD), write_strength_projection.T, decay_projection.T,
        query_weight, key_weight, value_weight, mixer_output_weight, gate_weight, up_weight,
        down_weight,
    )


def solution(mesh):
    torus = Mesh(mesh.devices.reshape(4, 4, 8, 2), ("ep_0", "ep_1", "tp_0", "tp_1"))
    placed = (
        P(EP_TP, None),
        P(),
        P(None, TP),
        P(None, TP),
        P(None, TP),
        P(),
        P(),
        P(TP),
        P(TP),
        P(EP, TP),
        P(),
        P(TP, None),
        P(EP_TP, None),
        P(),
        P(EP_TP, None),
        P(EP_TP, None),
        P(EP, None, TP),
        P(EP, None, TP),
        P(EP, TP, None),
    )
    return jax.shard_map(
        body,
        mesh=torus,
        in_specs=placed,
        out_specs=(P(EP_TP, None), P(EP_TP, None)),
        check_vma=False,
    )
```

```python
import functools

import jax
import jax.numpy as jnp
from jax import lax
from jax.experimental import pallas as pl
from jax.experimental.pallas import tpu as pltpu
from jax.sharding import Mesh
from jax.sharding import PartitionSpec as P

HEAD = 128
BLOCK = 128
EP = ("ep_0", "ep_1")
TP = ("tp_0", "tp_1")
EP_TP = ("ep_0", "ep_1", "tp_0", "tp_1")
MESH = pl.DeviceIdType.MESH

norm_eps = 1e-06
f32 = jnp.float32
bf16 = jnp.bfloat16


def mm(a, b):
    return jnp.dot(a.astype(bf16), b.astype(bf16), preferred_element_type=f32)


def mm_nt(a, b):
    return lax.dot_general(
        a.astype(bf16), b.astype(bf16), (((1,), (1,)), ((), ())), preferred_element_type=f32
    )


def silu(v):
    return v / (1.0 + jnp.exp(-v))


def project_pair(x, w_all, extra, speed, largest):
    p = jnp.dot(x, w_all, preferred_element_type=f32)
    q = silu(p[:, :HEAD])
    k = silu(p[:, HEAD : 2 * HEAD])
    k = k * lax.rsqrt(jnp.sum(k * k, axis=-1, keepdims=True) + 1e-06)
    v = silu(p[:, 2 * HEAD : 3 * HEAD])
    strength = largest / (1.0 + jnp.exp(-p[:, 3 * HEAD : 4 * HEAD]))
    raw = p[:, 4 * HEAD : 5 * HEAD]
    softplus = jnp.maximum(raw, 0.0) + jnp.log(1.0 + jnp.exp(-jnp.abs(raw)))
    return q, k, v, strength, extra - speed * softplus


def lockstep_invert(systems):
    row = lax.broadcasted_iota(jnp.int32, (BLOCK, BLOCK), 0)
    col = lax.broadcasted_iota(jnp.int32, (BLOCK, BLOCK), 1)
    apart = row ^ col
    eye = jnp.where(row == col, 1.0, 0.0)
    inverses = [eye - jnp.where(apart == 1, a, 0.0) for a in systems]
    size = 2
    while size < BLOCK:
        keep = (apart >= size) & (apart < 4 * size)
        xs = [a.astype(bf16) for a in inverses]
        ns = [mm(x, jnp.where(keep, a, 0.0)).astype(bf16) for x, a in zip(xs, systems)]
        ys = [a - mm(n, x) for a, n, x in zip(inverses, ns, xs)]
        squares = [mm(n, n) for n in ns]
        inverses = [y + mm(n2, y) for y, n2 in zip(ys, squares)]
        size *= 4
    return inverses


def block_maps(qs, ks, vs, strengths, log_decays):
    row = lax.broadcasted_iota(jnp.int32, (BLOCK, BLOCK), 0)
    col = lax.broadcasted_iota(jnp.int32, (BLOCK, BLOCK), 1)
    lower = jnp.where(row >= col, 1.0, 0.0).astype(bf16)
    parts = []
    for a in log_decays:
        high = a.astype(bf16)
        rest = a - high.astype(f32)
        middle = rest.astype(bf16)
        parts.append((high, middle, (rest - middle.astype(f32)).astype(bf16)))
    totals = [mm(lower, h) + mm(lower, m) + mm(lower, l) for h, m, l in parts]
    boths = [mm_nt(jnp.concatenate([q, k], axis=0), k) for q, k in zip(qs, ks)]
    decays = [jnp.exp(jnp.where(row >= col, a - a.T, -1e30)) for a in totals]
    scores = [b[:BLOCK] * d for b, d in zip(boths, decays)]
    systems = [
        jnp.where(row > col, b[BLOCK:] * s * d, 0.0) for b, s, d in zip(boths, strengths, decays)
    ]
    inverses = lockstep_invert(systems)
    growns = [jnp.exp(a) for a in totals]
    rights = [
        jnp.concatenate([s * g * k, s * v], axis=1)
        for s, g, k, v in zip(strengths, growns, ks, vs)
    ]
    solveds = [mm(a, b) for a, b in zip(inverses, rights)]
    lasts = [a[BLOCK - 1 : BLOCK, :] for a in totals]
    lefts = [
        jnp.concatenate([s, (k * jnp.exp(last - a)).T], axis=0)
        for s, k, last, a in zip(scores, ks, lasts, totals)
    ]
    joineds = [mm(a, b) for a, b in zip(lefts, solveds)]
    return [
        (q * g - j[:BLOCK, :HEAD], j[:BLOCK, HEAD:], j[BLOCK:, :HEAD], j[BLOCK:, HEAD:], jnp.exp(last))
        for q, g, j, last in zip(qs, growns, joineds, lasts)
    ]


def pairs_maps(xs, w_all, extras, speed, largest):
    columns = [[], [], [], [], []]
    for x, extra in zip(xs, extras):
        for list_, a in zip(columns, project_pair(x, w_all, extra, speed, largest)):
            list_ += [a[:BLOCK], a[BLOCK:]]
    blocks = block_maps(*columns)
    results = []
    for a, b in zip(blocks[0::2], blocks[1::2]):
        (qa, oa, ga, sa, da), (qb, ob, gb, sb, db) = a, b
        t = mm(jnp.concatenate([gb, qb], axis=0), jnp.concatenate([ga, sa], axis=1))
        g = db * ga + da * gb - t[:BLOCK, :HEAD]
        s = db * sa - t[:BLOCK, HEAD:] + sb
        qb = da * qb - t[BLOCK:, :HEAD]
        ob = t[BLOCK:, HEAD:] + ob
        results.append(
            (jnp.concatenate([qa, qb], axis=0), jnp.concatenate([oa, ob], axis=0), g, s, da * db)
        )
    return results


CHIPS = 8
RING = 4
EPS = RING * RING
SLOTS = 2
ROWS = EPS * SLOTS
MSG = 8


def normed(x, gain):
    widened = x.astype(f32)
    scaled = widened * lax.rsqrt(jnp.mean(widened * widened, axis=-1, keepdims=True) + norm_eps)
    return (scaled * gain).astype(bf16)


def three_parts(a):
    high = a.astype(bf16)
    rest = a - high.astype(f32)
    middle = rest.astype(bf16)
    return high, middle, (rest - middle.astype(f32)).astype(bf16)


def layer_kernel(
    xm_ref, mgain_ref, xe_ref, egain_ref, routes_ref, share_ref, extra_ref, speed_ref, largest_ref,
    hgain_ref, wst_ref, wdt_ref, wq_ref, wk_ref, wv_ref, wo_ref, gate_ref, up_ref, down_ref,
    mix_ref, exp_ref,
    w_all, gate_s, up_s, down_s, xb, eb, lhs_s, g_s, s_s, o_s, d_s, ps_s, qh_s, oh_s,
    row_maps, col_maps, total_s, heads_out, heads_in, wg,
    msg_out, msg_in, pb, pr, ss, rl, ret_out, ret_in,
    load_sem, ring_send, ring_recv, msg_send, msg_recv, ret_send, ret_recv, w_send, w_recv,
    pb_send, pb_recv, rs_send, rs_recv, map_send, row_recv, col_recv, head_send, head_recv,
):
    y, x = lax.axis_index("ep_0"), lax.axis_index("ep_1")
    z, c = lax.axis_index("tp_0"), lax.axis_index("tp_1")
    e = y * RING + x
    t = z * 2 + c
    other = 1 - c
    a, b = jnp.where(c == 0, y, x), jnp.where(c == 0, x, y)
    f = a * RING + b

    def at_tp(chip, core):
        return {"tp_0": chip, "tp_1": core}

    def at_ep(o):
        return {"ep_0": o // RING, "ep_1": o % RING}

    def remote(src, dst, send, recv, where):
        return pltpu.make_async_remote_copy(
            src, dst, send, recv, device_id=where, device_id_type=MESH
        )

    loads = [
        pltpu.make_async_copy(wq_ref, w_all.at[:, pl.ds(0, HEAD)], load_sem.at[0]),
        pltpu.make_async_copy(wk_ref, w_all.at[:, pl.ds(HEAD, HEAD)], load_sem.at[1]),
        pltpu.make_async_copy(wv_ref, w_all.at[:, pl.ds(2 * HEAD, HEAD)], load_sem.at[2]),
        pltpu.make_async_copy(gate_ref.at[0], gate_s, load_sem.at[3]),
        pltpu.make_async_copy(up_ref.at[0], up_s, load_sem.at[4]),
        pltpu.make_async_copy(down_ref.at[0], down_s, load_sem.at[5]),
        pltpu.make_async_copy(
            wo_ref.at[:, pl.ds(pl.multiple_of(e * HEAD, HEAD), HEAD)], wg.at[c, f, z], load_sem.at[6]
        ),
    ]
    for copy in loads:
        copy.start()

    barrier = pltpu.get_barrier_semaphore()
    for j in range(1, 16):
        o = (t + j) % 16
        pl.semaphore_signal(barrier, 1, device_id=at_tp(o // 2, o % 2), device_id_type=MESH)
        pl.semaphore_signal(barrier, 1, device_id=at_ep((e + j) % EPS), device_id_type=MESH)

    xb[t] = normed(xm_ref[...], mgain_ref[...])

    place = lax.broadcasted_iota(jnp.int32, (EPS * MSG, MSG), 0)
    first = jnp.where(place // MSG == routes_ref[0:1, :], 1.0, 0.0)
    second = jnp.where(place // MSG == routes_ref[1:2, :], 1.0, 0.0)
    named = first + second
    token = lax.broadcasted_iota(jnp.int32, (EPS * MSG, MSG), 1)
    before = jnp.zeros((EPS * MSG, MSG), f32)
    for i in range(MSG - 1):
        before = before + jnp.where(token > i, named[:, i : i + 1], 0.0)
    fills = jnp.where(before == (place % MSG).astype(f32), named, 0.0)
    shares = (fills * (first * share_ref[0:1, :] + second * share_ref[1:2, :])).T
    xn = normed(xe_ref[...], egain_ref[...])
    messages = mm(fills, xn)
    for o in range(EPS):
        msg_out[o] = messages[o * MSG : (o + 1) * MSG].astype(bf16)
    pl.semaphore_wait(barrier, 30)

    def ring_copy(block, part, way, where):
        half = BLOCK // 2
        piece = (
            xb.at[block, pl.ds(0, half)],
            xb.at[block, pl.ds(half, half)],
            eb.at[block],
            wg.at[c, f, block // 2],
        )[part]
        return remote(
            piece, piece, ring_send.at[block, part, way], ring_recv.at[block, part], where
        )

    up_chip, down_chip = (z + 1) % CHIPS, (z + CHIPS - 1) % CHIPS

    def send_own(part):
        ring_copy(t, part, 0, at_tp(up_chip, c)).start()
        ring_copy(t, part, 1, at_tp(down_chip, c)).start()
        if part < 3:
            ring_copy(t, part, 2, at_tp(z, other)).start()

    def arrived(block, part):
        ring_copy(block, part, 0, at_tp(up_chip, c)).wait_recv()

    def relay(k, part):
        behind, ahead = (z + CHIPS - k) % CHIPS, (z + k) % CHIPS
        arrived(behind * 2 + c, part)

        @pl.when((k < 3) | (c == 0))
        def _():
            ring_copy(behind * 2 + c, part, 0, at_tp(up_chip, c)).start()

        if part < 3:
            ring_copy(behind * 2 + c, part, 2, at_tp(z, other)).start()
        arrived(ahead * 2 + c, part)

        @pl.when((k < 3) | (c == 1))
        def _():
            ring_copy(ahead * 2 + c, part, 1, at_tp(down_chip, c)).start()

        if part < 3:
            ring_copy(ahead * 2 + c, part, 2, at_tp(z, other)).start()

    loads[6].wait()
    send_own(3)
    send_own(0)
    msg_copies = []
    for j in range(1, EPS):
        o = (e + j) % EPS
        msg_copies.append(
            remote(msg_out.at[o], msg_in.at[e], msg_send.at[j], msg_recv.at[e], at_ep(o))
        )
    for copy in msg_copies:
        copy.start()
    msg_in[e] = msg_out[e]

    heads = wst_ref.shape[0]
    pick = jnp.where(lax.broadcasted_iota(jnp.int32, (heads, HEAD), 0) == t, 1.0, 0.0)
    w_all[:, 3 * HEAD : 4 * HEAD] = mm(wst_ref[...].astype(f32).T, pick).astype(bf16)
    w_all[:, 4 * HEAD : 5 * HEAD] = mm(wdt_ref[...].astype(f32).T, pick).astype(bf16)

    relay(1, 3)
    send_own(1)

    for j in range(1, EPS):
        o = (e + j) % EPS
        remote(msg_out.at[0], msg_in.at[o], msg_send.at[0], msg_recv.at[o], at_ep(o)).wait_recv()
    landed = jnp.concatenate([msg_in[o].astype(f32) for o in range(EPS)], axis=0)
    slot = lax.broadcasted_iota(jnp.int32, (ROWS, EPS * MSG), 0)
    line = lax.broadcasted_iota(jnp.int32, (ROWS, EPS * MSG), 1)
    squeeze = jnp.where(
        (line // MSG == slot // SLOTS) & (line % MSG == slot % SLOTS), 1.0, 0.0
    )
    eb[t] = mm(squeeze, landed).astype(bf16)
    for copy in loads[:3]:
        copy.wait()
    send_own(2)

    speed, largest = speed_ref[0], largest_ref[0]

    def extra_of(chip):
        rows = [
            jnp.broadcast_to(extra_ref[chip * 2 + i], (HEAD, BLOCK)).T for i in range(2)
        ]
        return jnp.concatenate(rows, axis=0)

    def span_group(chips):
        xs = [jnp.concatenate([xb[chip * 2], xb[chip * 2 + 1]], axis=0) for chip in chips]
        extras = [extra_of(chip) for chip in chips]
        for chip, (q, o, g, s, d) in zip(chips, pairs_maps(xs, w_all[...], extras, speed, largest)):
            lhs_s[chip, :HEAD] = g.astype(bf16)
            lhs_s[chip, HEAD:] = q.astype(bf16)
            o_s[chip] = o
            g_s[chip] = g
            s_s[chip] = s
            d_s[chip] = jnp.broadcast_to(d, (8, HEAD))

    def pb_copy(chip):
        return remote(
            pb.at[chip, other], pr.at[chip], pb_send.at[chip], pb_recv.at[chip], at_tp(z, other)
        )

    def expert_group(chips):
        rows = jnp.concatenate(
            [eb[chip * 2 + i] for chip in chips for i in range(2)], axis=0
        )
        gated = mm_nt(rows, gate_s[...])
        raised = mm_nt(rows, up_s[...])
        hidden = (silu(gated) * raised).astype(bf16)
        width = 1024
        for n in range(0, down_s.shape[1], width):
            part = jnp.dot(hidden, down_s[:, n : n + width], preferred_element_type=f32)
            for i, chip in enumerate(chips):
                for core in range(2):
                    start = (i * 2 + core) * ROWS
                    pb[chip, core, :, n : n + width] = part[start : start + ROWS].astype(bf16)
        for chip in chips:
            pb_copy(chip).start()

    def rs_copy(chip):
        return remote(ss.at[chip], rl.at[z], rs_send.at[chip], rs_recv.at[z], at_tp(chip, c))

    def add_partner(chip):
        pb_copy(chip).wait_recv()
        ss[chip] = (pb[chip, c].astype(f32) + pr[chip].astype(f32)).astype(bf16)

    arrived(z * 2 + other, 0)
    arrived(z * 2 + other, 1)
    span_group([z])
    relay(2, 3)
    for copy in loads[3:6]:
        copy.wait()
    arrived(z * 2 + other, 2)
    expert_group([z])

    def w_copy(stage, side, take):
        moved = (1 if side == 0 else RING - 1)
        if stage < 2:
            ta, tb = a, (b + moved) % RING
        else:
            ta, tb = (a + moved) % RING, b
        where = {"ep_0": jnp.where(c == 0, ta, tb), "ep_1": jnp.where(c == 0, tb, ta)}
        index = CHIPS + 2 * stage + side
        return remote(take, take, w_send.at[index], w_recv.at[index], where)

    def w_piece(stage, side, sender):
        half = CHIPS // 2
        if stage == 0:
            return wg.at[c, a * RING + (b + sender) % RING]
        if stage == 1:
            source = (b + sender + (RING - 1 if side == 0 else 1)) % RING
            return wg.at[c, a * RING + source, pl.ds(side * half, half)]
        if stage == 2:
            return wg.at[c, pl.ds((a + sender) % RING * RING, RING)]
        source = (a + sender + (RING - 1 if side == 0 else 1)) % RING
        return wg.at[c, pl.ds(source * RING + side * (RING // 2), RING // 2)]

    def w_send_stage(stage):
        for side in range(2):
            w_copy(stage, side, w_piece(stage, side, 0)).start()

    def w_wait_stage(stage):
        for side in range(2):
            sender = RING - 1 if side == 0 else 1
            w_copy(stage, side, w_piece(stage, side, sender)).wait_recv()

    far = (z + 4) % CHIPS

    for k in range(1, 4):
        behind, ahead = (z + CHIPS - k) % CHIPS, (z + k) % CHIPS
        relay(k, 0)
        relay(k, 1)
        for chip in (behind, ahead):
            for part in range(2):
                arrived(chip * 2 + other, part)
        span_group([behind, ahead])
        relay(k, 2)
        if k == 1:
            relay(3, 3)
        if k == 2:
            arrived(far * 2 + c, 3)
            w_send_stage(0)
        if k == 3:
            w_wait_stage(1)
            w_send_stage(2)
        for chip in (behind, ahead):
            arrived(chip * 2 + other, 2)
        expert_group([behind, ahead])
        if k == 2:
            w_wait_stage(0)
            w_send_stage(1)

    for j in range(CHIPS):
        if j != 4:
            chip = (z + j) % CHIPS
            add_partner(chip)
            if j:
                rs_copy(chip).start()
    for part in range(2):
        arrived(far * 2 + c, part)
        ring_copy(far * 2 + c, part, 2, at_tp(z, other)).start()
    for part in range(2):
        arrived(far * 2 + other, part)
    span_group([far])

    g = jnp.zeros((HEAD, HEAD), f32)
    s = jnp.zeros((HEAD, HEAD), f32)
    d = jnp.ones((1, HEAD), f32)
    for chip in range(CHIPS):
        rows = slice(chip * 2 * BLOCK, (chip + 1) * 2 * BLOCK)
        lhs = lhs_s[chip]
        m = mm(lhs, jnp.concatenate([g, s], axis=1))
        qh_s[rows, :] = (d * lhs[HEAD:].astype(f32) - m[HEAD:, :HEAD]).astype(bf16)
        oh_s[rows, :] = m[HEAD:, HEAD:] + o_s[chip]
        dz = d_s[chip, 0:1, :]
        g, s = dz * g + d * g_s[chip] - m[:HEAD, :HEAD], dz * s - m[:HEAD, HEAD:] + s_s[chip]
        d = d * dz
    row = lax.broadcasted_iota(jnp.int32, (HEAD, HEAD), 0)
    col = lax.broadcasted_iota(jnp.int32, (HEAD, HEAD), 1)
    own_map = jnp.concatenate([jnp.where(row == col, d, 0.0) - g, s], axis=1).astype(bf16)
    ps_s[...] = own_map
    map_copies = []
    for j in range(1, RING):
        map_copies.append(
            remote(
                ps_s, row_maps.at[x], map_send.at[j], row_recv.at[x], {"ep_1": (x + j) % RING}
            )
        )
    for copy in map_copies:
        copy.start()
    row_maps[x] = own_map
    w_wait_stage(2)
    w_send_stage(3)

    arrived(far * 2 + c, 2)
    ring_copy(far * 2 + c, 2, 2, at_tp(z, other)).start()
    arrived(far * 2 + other, 2)
    expert_group([far])

    for j in range(1, RING):
        o = (x + j) % RING
        remote(ps_s, row_maps.at[o], map_send.at[0], row_recv.at[o], {"ep_1": o}).wait_recv()
    whole = row_maps[0]
    mine = whole
    for k in range(1, RING):
        mine = jnp.where(x == k, whole, mine)
        later = row_maps[k]
        m = mm(later[:, :HEAD], whole)
        whole = jnp.concatenate(
            [m[:, :HEAD], m[:, HEAD:] + later[:, HEAD:].astype(f32)], axis=1
        ).astype(bf16)
    total_s[...] = whole
    total_copies = []
    for j in range(1, RING):
        total_copies.append(
            remote(
                total_s, col_maps.at[y], map_send.at[RING + j], col_recv.at[y],
                {"ep_0": (y + j) % RING},
            )
        )
    for copy in total_copies:
        copy.start()
    col_maps[y] = whole

    add_partner(far)
    rs_copy(far).start()

    for j in range(1, RING):
        o = (y + j) % RING
        remote(
            total_s, col_maps.at[o], map_send.at[0], col_recv.at[o], {"ep_0": o}
        ).wait_recv()
    memory = jnp.zeros((HEAD, HEAD), f32)
    for k in range(RING - 1):
        earlier = col_maps[k]
        moved = earlier[:, HEAD:].astype(f32)
        if k:
            moved = moved + mm(earlier[:, :HEAD], memory)
        memory = jnp.where(k < y, moved, memory)
    moved = mm(mine[:, :HEAD], memory) + mine[:, HEAD:].astype(f32)
    memory = jnp.where(x > 0, moved, memory).astype(bf16)

    w_wait_stage(3)
    w_half = remote(
        wg.at[c], wg.at[c], w_send.at[CHIPS + 8], w_recv.at[CHIPS + 8],
        at_tp(z, other),
    )
    w_half.start()

    hgain = hgain_ref[...]
    for chip in range(CHIPS):
        rows = slice(chip * 2 * BLOCK, (chip + 1) * 2 * BLOCK)
        o = mm(qh_s[rows, :], memory) + oh_s[rows, :]
        o = o * lax.rsqrt(jnp.mean(o * o, axis=-1, keepdims=True) + norm_eps)
        heads_out[rows, :] = (o * hgain).astype(bf16)
    own_cols = pl.ds(pl.multiple_of(t * HEAD, HEAD), HEAD)
    head_copies = []
    for j in range(1, 16):
        o = (t + j) % 16
        rows = pl.ds(pl.multiple_of(o * BLOCK, BLOCK), BLOCK)
        head_copies.append(
            remote(
                heads_out.at[rows, :], heads_in.at[:, own_cols], head_send.at[j], head_recv.at[t],
                at_tp(o // 2, o % 2),
            )
        )
    for copy in head_copies:
        copy.start()
    heads_in[:, own_cols] = heads_out[pl.ds(pl.multiple_of(t * BLOCK, BLOCK), BLOCK), :]

    total = ss[z].astype(f32)
    for j in range(1, CHIPS):
        o = (z + j) % CHIPS
        remote(ss.at[0], rl.at[o], rs_send.at[o], rs_recv.at[o], at_tp(o, c)).wait_recv()
        total = total + rl[o].astype(f32)
    spread_line = lax.broadcasted_iota(jnp.int32, (EPS * MSG, ROWS), 0)
    spread_slot = lax.broadcasted_iota(jnp.int32, (EPS * MSG, ROWS), 1)
    spread = jnp.where(
        (spread_line // MSG == spread_slot // SLOTS)
        & (spread_line % MSG == spread_slot % SLOTS),
        1.0,
        0.0,
    )
    returning = mm(spread, total)
    for o in range(EPS):
        ret_out[o] = returning[o * MSG : (o + 1) * MSG].astype(bf16)
    ret_copies = []
    for j in range(1, EPS):
        o = (e + j) % EPS
        ret_copies.append(
            remote(ret_out.at[o], ret_in.at[e], ret_send.at[j], ret_recv.at[e], at_ep(o))
        )
    for copy in ret_copies:
        copy.start()
    ret_in[e] = ret_out[e]

    remote(
        wg.at[other], wg.at[other], w_send.at[0], w_recv.at[CHIPS + 8], at_tp(z, other)
    ).wait_recv()
    for j in range(1, 16):
        o = (t + j) % 16
        cols = pl.ds(pl.multiple_of(o * HEAD, HEAD), HEAD)
        remote(
            heads_out.at[pl.ds(0, BLOCK), :], heads_in.at[:, cols], head_send.at[0],
            head_recv.at[o], at_tp(o // 2, o % 2),
        ).wait_recv()
    def piece(core, o):
        return o if core == 0 else o % RING * RING + o // RING

    for pair in range(EPS // 2):
        weight = jnp.concatenate(
            [
                jnp.concatenate(
                    [
                        wg[core, piece(core, 2 * pair + i), chip]
                        for chip in range(CHIPS)
                        for core in range(2)
                    ],
                    axis=0,
                )
                for i in range(2)
            ],
            axis=1,
        )
        mix_ref[:, pair * 2 * HEAD : (pair + 1) * 2 * HEAD] = jnp.dot(
            heads_in[...], weight, preferred_element_type=f32
        ).astype(bf16)

    for j in range(1, EPS):
        o = (e + j) % EPS
        remote(ret_out.at[0], ret_in.at[o], ret_send.at[0], ret_recv.at[o], at_ep(o)).wait_recv()
    results = jnp.concatenate([ret_in[o].astype(f32) for o in range(EPS)], axis=0).astype(bf16)
    out = sum(jnp.dot(a, results, preferred_element_type=f32) for a in three_parts(shares))
    exp_ref[...] = out.astype(bf16)

    for copy in (
        msg_copies + [w_half] + map_copies + total_copies
        + head_copies + ret_copies
    ):
        copy.wait_send()
    for part in range(4):
        ring_copy(t, part, 0, at_tp(up_chip, c)).wait_send()
        ring_copy(t, part, 1, at_tp(down_chip, c)).wait_send()
        for k in range(1, 4):
            behind, ahead = (z + CHIPS - k) % CHIPS, (z + k) % CHIPS

            @pl.when((k < 3) | (c == 0))
            def _():
                ring_copy(behind * 2 + c, part, 0, at_tp(up_chip, c)).wait_send()

            @pl.when((k < 3) | (c == 1))
            def _():
                ring_copy(ahead * 2 + c, part, 1, at_tp(down_chip, c)).wait_send()

        if part < 3:
            for j in range(CHIPS):
                ring_copy((z + j) % CHIPS * 2 + c, part, 2, at_tp(z, other)).wait_send()
    for stage in range(4):
        for side in range(2):
            w_copy(stage, side, w_piece(stage, side, 0)).wait_send()
    for chip in range(CHIPS):
        pb_copy(chip).wait_send()
    for j in range(1, CHIPS):
        rs_copy((z + j) % CHIPS).wait_send()


def body(
    mixer_input_rows,
    mixer_norm_gain,
    query_weight,
    key_weight,
    value_weight,
    write_strength_projection,
    decay_projection,
    head_decay_speed,
    largest_write_strength,
    extra_log_decay,
    head_norm_gain,
    mixer_output_weight,
    expert_input_rows,
    expert_norm_gain,
    routes,
    expert_route_weight,
    gate_weight,
    up_weight,
    down_weight,
):
    rows, model = mixer_input_rows.shape
    tokens = expert_input_rows.shape[0]
    hidden = gate_weight.shape[2]
    span = extra_log_decay.shape[0]
    blocks = span // BLOCK
    vm = pl.BlockSpec(memory_space=pltpu.VMEM)
    sm = pl.BlockSpec(memory_space=pltpu.SMEM)
    hbm = pl.BlockSpec(memory_space=pltpu.HBM)
    dma = pltpu.SemaphoreType.DMA
    return pl.pallas_call(
        layer_kernel,
        out_shape=(
            jax.ShapeDtypeStruct((rows, model), bf16),
            jax.ShapeDtypeStruct((tokens, model), bf16),
        ),
        in_specs=[vm] * 7 + [sm] * 2 + [vm] * 3 + [hbm] * 7,
        out_specs=(vm, vm),
        scratch_shapes=[
            pltpu.VMEM((model, 5 * HEAD), bf16),
            pltpu.VMEM((hidden, model), bf16),
            pltpu.VMEM((hidden, model), bf16),
            pltpu.VMEM((hidden, model), bf16),
            pltpu.VMEM((blocks, BLOCK, model), bf16),
            pltpu.VMEM((blocks, ROWS, model), bf16),
            pltpu.VMEM((CHIPS, 3 * HEAD, HEAD), bf16),
            pltpu.VMEM((CHIPS, HEAD, HEAD), f32),
            pltpu.VMEM((CHIPS, HEAD, HEAD), f32),
            pltpu.VMEM((CHIPS, 2 * BLOCK, HEAD), f32),
            pltpu.VMEM((CHIPS, 8, HEAD), f32),
            pltpu.VMEM((HEAD, 2 * HEAD), bf16),
            pltpu.VMEM((span, HEAD), bf16),
            pltpu.VMEM((span, HEAD), f32),
            pltpu.VMEM((RING, HEAD, 2 * HEAD), bf16),
            pltpu.VMEM((RING, HEAD, 2 * HEAD), bf16),
            pltpu.VMEM((HEAD, 2 * HEAD), bf16),
            pltpu.VMEM((span, HEAD), bf16),
            pltpu.VMEM((BLOCK, model), bf16),
            pltpu.VMEM((2, EPS, CHIPS, HEAD, HEAD), bf16),
            pltpu.VMEM((EPS, MSG, model), bf16),
            pltpu.VMEM((EPS, MSG, model), bf16),
            pltpu.VMEM((CHIPS, 2, ROWS, model), bf16),
            pltpu.VMEM((CHIPS, ROWS, model), bf16),
            pltpu.VMEM((CHIPS, ROWS, model), bf16),
            pltpu.VMEM((CHIPS, ROWS, model), bf16),
            pltpu.VMEM((EPS, MSG, model), bf16),
            pltpu.VMEM((EPS, MSG, model), bf16),
            dma((7,)),
            dma((16, 4, 3)),
            dma((16, 4)),
            dma((EPS,)),
            dma((EPS,)),
            dma((EPS,)),
            dma((EPS,)),
            dma((CHIPS + 9,)),
            dma((CHIPS + 9,)),
            dma((CHIPS,)),
            dma((CHIPS,)),
            dma((CHIPS,)),
            dma((CHIPS,)),
            dma((2 * RING,)),
            dma((RING,)),
            dma((RING,)),
            dma((16,)),
            dma((16,)),
        ],
        compiler_params=pltpu.CompilerParams(
            vmem_limit_bytes=60 * 1024 * 1024, collective_id=1, has_side_effects=True
        ),
        cost_estimate=pl.CostEstimate(
            flops=10_000_000_000, bytes_accessed=32 * 1024 * 1024, transcendentals=0
        ),
        name="layer",
    )(
        mixer_input_rows, mixer_norm_gain.reshape(1, model), expert_input_rows,
        expert_norm_gain.reshape(1, model), routes.T, expert_route_weight.T,
        extra_log_decay.reshape(blocks, 1, BLOCK), head_decay_speed, largest_write_strength,
        head_norm_gain.reshape(1, HEAD), write_strength_projection.T, decay_projection.T,
        query_weight, key_weight, value_weight, mixer_output_weight,
        jnp.swapaxes(gate_weight, 1, 2), jnp.swapaxes(up_weight, 1, 2), down_weight,
    )


def solution(mesh):
    torus = Mesh(mesh.devices.reshape(4, 4, 8, 2), ("ep_0", "ep_1", "tp_0", "tp_1"))
    placed = (
        P(EP_TP, None),
        P(),
        P(None, TP),
        P(None, TP),
        P(None, TP),
        P(),
        P(),
        P(TP),
        P(TP),
        P(EP, TP),
        P(),
        P(TP, None),
        P(EP_TP, None),
        P(),
        P(EP_TP, None),
        P(EP_TP, None),
        P(EP, None, TP),
        P(EP, None, TP),
        P(EP, TP, None),
    )
    return jax.shard_map(
        body,
        mesh=torus,
        in_specs=placed,
        out_specs=(P(EP_TP, None), P(EP_TP, None)),
        check_vma=False,
    )
```
